256 devices in a mesh: sp: 64 (over z, y, core), tp: 4 (over x).
Axes of the slice: x: 4, y: 4, z: 8, core: 2. Of those that a mesh axis runs over, the one named last changes fastest.
Arguments:
- residual: bfloat16 [16384, 2048], P('sp'), may hold values from -6 to 6
- queries: bfloat16 [16384, 8, 128], P('sp', 'tp'), may hold values from -100 to 100
- keys: bfloat16 [16384, 8, 128], P('sp', 'tp'), may hold values from -60 to 60
- values: bfloat16 [16384, 8, 128], P('sp', 'tp'), may hold values from -6 to 6
- documents: int32 [16384], P('sp'), may hold values from 0 to 7, never falling along the last dimension, each value on 1 to 8192 neighbouring positions
- lambdas: float32 [8], P('tp'), may hold values from 0.3 to 0.8
- head_gain: float32 [8, 128], P('tp'), may hold values from 0.1 to 1.9
- out_weight: bfloat16 [1024, 2048], replicated, may hold values from -0.1875 to 0.1875
- mix_gain: float32 [2048], replicated, may hold values from 0.1 to 1.9
- pre_gain: float32 [2048], replicated, may hold values from 0.1 to 1.9
- gate_weight: bfloat16 [2048, 3072], P('sp', 'tp'), may hold values from -0.125 to 0.125
- value_weight: bfloat16 [2048, 3072], P('sp', 'tp'), may hold values from -0.125 to 0.125
- gate_taps: float32 [3, 3072], P(None, 'tp'), may hold values from -3 to 3
- value_taps: float32 [3, 3072], P(None, 'tp'), may hold values from -3 to 3
- down_weight: bfloat16 [2048, 3072], P('sp', 'tp'), may hold values from -0.109375 to 0.109375
- mlp_gain: float32 [2048], replicated, may hold values from 0.1 to 1.9
Outputs:
- out: bfloat16 [16384, 2048], P('sp')
The draws below stay inside these ranges and needn't reach their ends.
All inputs are finite; a program needn't handle non-finite values.
Results may differ from the reference program's by a relative error of at most 0.015.
Values may be sent and summed in bfloat16 or wider, within the bound.
No kernel may reach another device: no remote copies, remote signals or barrier semaphores. Data moves between devices by JAX's collectives and lax.ppermute only.
A program may use at most 128 MiB of HBM per device.

```python
import math
import jax
import jax.numpy as jnp
import numpy as np
from jax import lax

D = 2048
HEADS = 8
QK = 64
HEAD_DIM = 128
FF = 3072
TAPS = 3
DOCS = 8
TOKENS = 16384
N_TP = 4


def draw_queries(key, part):
    random_part = jnp.clip(1.3 * jax.random.normal(jax.random.fold_in(key, 1), (TOKENS, HEADS, 2, QK), jnp.float32), -6.5, 6.5)
    return random_part.reshape(TOKENS, HEADS, 2 * QK).astype(jnp.bfloat16)


def draw_keys(key, part):
    random_part = jnp.clip(1.3 * jax.random.normal(jax.random.fold_in(key, 2), (TOKENS, HEADS, 2, QK), jnp.float32), -6.5, 6.5)
    return random_part.reshape(TOKENS, HEADS, 2 * QK).astype(jnp.bfloat16)


def block_scale(stream_key, shape, pieces, least, top_value):
    def one(position, shards_of):
        heights = jax.random.uniform(jax.random.fold_in(jax.random.fold_in(stream_key, 6), position), (shards_of,), jnp.float32, least / len(pieces), top_value / len(pieces))
        return jnp.repeat(jnp.exp(heights), shape[position] // shards_of).reshape((-1,) + (1,) * (len(shape) - position - 1))

    level = one(*pieces[0])
    for cut in pieces[1:]:
        level = level * one(*cut)
    return level


def length_profile(count, total, limit, lean):
    portions = [(1 << 20) // math.isqrt(standing ** lean) + 1 for standing in range(2, count + 1)]
    rest, given = total - limit - (count - 1), [1] * (count - 1)
    while rest > 0:
        movable = [i for i in range(count - 1) if given[i] < limit]
        pool, left = sum([portions[i] for i in movable]), rest
        for i in movable:
            more = min(limit - given[i], max(1, left * portions[i] // pool), rest)
            given[i] = given[i] + more
            rest = rest - more
    return np.array([limit] + given)


def ragged(rng, number_of, total, most, skew):
    if number_of == 2:
        one = jax.random.randint(rng, (), max(1, total - most), min(most, total - 1) + 1)
        return jnp.stack([one, total - one])
    sizes = jnp.asarray(length_profile(number_of, total, most, skew), jnp.int32)
    pairs = (number_of - 1) // 2
    giver, receiver = sizes[1:1 + 2 * pairs:2], sizes[2:2 + 2 * pairs:2]
    room = jnp.minimum(giver - 1, most - receiver)
    shifted = jax.random.randint(jax.random.fold_in(rng, 1), (pairs,), 0, 1 << 20) % (room + 1)
    sizes = sizes.at[1:1 + 2 * pairs:2].set(giver - shifted).at[2:2 + 2 * pairs:2].set(receiver + shifted)
    return sizes[jax.random.permutation(jax.random.fold_in(rng, 2), number_of)]


def normal_values(key, extent, deviation, most, cuts=(), kind=jnp.bfloat16):
    values = jax.random.normal(key, extent, jnp.float32) * deviation
    if len(cuts) > 0:
        values = block_scale(key, extent, cuts, -0.22, 0.18) * values
    return jnp.clip(values, min=-most, max=most).astype(kind)


def setup_inputs(seed: int = 0) -> dict:
    splits = jax.random.split(jax.random.key(seed), 17)
    residual = normal_values(splits[0], (TOKENS, D), 1.0, 6.0, ((0, 64),))
    queries = draw_queries(jax.random.fold_in(splits[16], 71), 0)
    keys = draw_keys(jax.random.fold_in(splits[16], 71), 0)
    values = normal_values(splits[3], (TOKENS, HEADS, HEAD_DIM), 1.0, 6.0, ((0, 64), (1, 4)))
    documents = jnp.searchsorted(jnp.cumsum(ragged(splits[4], DOCS, TOKENS, TOKENS // 2, 0)), jnp.arange(TOKENS), side="right").astype(jnp.int32)
    lambdas = jnp.clip(0.3 + 0.5 * jax.random.uniform(splits[5], (HEADS,), jnp.float32) ** block_scale(splits[5], (HEADS,), ((0, 4),), -0.2, 0.2), 0.3, 0.8)
    head_gain = jnp.clip(1.0 + 0.18 * jax.random.normal(splits[6], (HEADS, HEAD_DIM), jnp.float32), 0.1, 1.9)
    out_weight = normal_values(splits[7], (HEADS * HEAD_DIM, D), (HEADS * HEAD_DIM) ** -0.5, 0.1875)
    mix_gain = jnp.clip(1.0 + 0.18 * jax.random.normal(splits[8], (D,), jnp.float32), 0.1, 1.9)
    pre_gain = jnp.clip(1.0 + 0.18 * jax.random.normal(splits[9], (D,), jnp.float32), 0.1, 1.9)
    gate_weight = normal_values(splits[10], (D, FF), D ** -0.5, 0.125, ((0, 64), (1, 4)))
    value_weight = normal_values(splits[11], (D, FF), D ** -0.5, 0.125, ((0, 64), (1, 4)))
    gate_taps = normal_values(splits[12], (TAPS, FF), 0.577, 3.0, ((1, 4),), jnp.float32)
    value_taps = normal_values(splits[13], (TAPS, FF), 0.577, 3.0, ((1, 4),), jnp.float32)
    down_weight = normal_values(splits[14], (D, FF), FF ** -0.5, 0.109375, ((0, 64), (1, 4)))
    mlp_gain = jnp.clip(1.0 + 0.18 * jax.random.normal(splits[15], (D,), jnp.float32), 0.1, 1.9)
    return dict(residual=residual, queries=queries, keys=keys, values=values, documents=documents, lambdas=lambdas, head_gain=head_gain, out_weight=out_weight, mix_gain=mix_gain, pre_gain=pre_gain, gate_weight=gate_weight, value_weight=value_weight, gate_taps=gate_taps, value_taps=value_taps, down_weight=down_weight, mlp_gain=mlp_gain)


epsilon = 1e-06

def rms_scale(values_in, gain):
    return values_in * lax.rsqrt(lax.optimization_barrier(jnp.mean(values_in * values_in, axis=-1, keepdims=True)) + epsilon) * gain

def reference(residual, queries, keys, values, documents, lambdas, head_gain, out_weight, mix_gain, pre_gain, gate_weight, value_weight, gate_taps, value_taps, down_weight, mlp_gain):
    query_block = math.gcd(TOKENS, 256)
    queries_wide = queries.astype(jnp.float32)
    keys_wide = keys.astype(jnp.float32)
    values_wide = values.astype(jnp.float32)
    positions = jnp.arange(TOKENS, dtype=jnp.int32)
    score_scale = QK ** (-0.5)

    def one_block(number):
        first_row = number * query_block
        query_rows = lax.dynamic_slice_in_dim(queries_wide, first_row, query_block, 0)
        query_pos = first_row + jnp.arange(query_block, dtype=jnp.int32)
        query_docs = lax.dynamic_slice_in_dim(documents, first_row, query_block, 0)
        allowed = (positions[None, :] <= query_pos[:, None]) & (documents[None, :] == query_docs[:, None])
        results = []
        for map_index in range(2):
            query_part = query_rows[:, :, map_index * QK:(map_index + 1) * QK]
            key_part = keys_wide[:, :, map_index * QK:(map_index + 1) * QK]
            scores = jnp.einsum('qhd,khd->hqk', query_part, key_part) * score_scale
            scores = jnp.where(allowed[None], scores, -jnp.inf)
            probs = jax.nn.softmax(scores, axis=-1).astype(jnp.bfloat16)
            probs = lax.optimization_barrier(probs).astype(jnp.float32)
            results.append(jnp.einsum('hqk,khe->qhe', probs, values_wide))
        return results[0] - lambdas[None, :, None] * results[1]
    heads = lax.map(one_block, jnp.arange(TOKENS // query_block, dtype=jnp.int32))
    heads = heads.reshape(TOKENS, HEADS, HEAD_DIM)
    normed = rms_scale(heads, head_gain[None]).astype(jnp.bfloat16).reshape(TOKENS, HEADS * HEAD_DIM)
    mixed = jnp.dot(normed, out_weight, preferred_element_type=jnp.float32)
    stream = residual.astype(jnp.float32) + rms_scale(mixed, mix_gain)
    normal_input = rms_scale(stream, pre_gain).astype(jnp.bfloat16)
    gate_pre = jnp.dot(normal_input, gate_weight, preferred_element_type=jnp.float32).astype(jnp.bfloat16)
    value_pre = jnp.dot(normal_input, value_weight, preferred_element_type=jnp.float32).astype(jnp.bfloat16)
    reach = TAPS - 1
    earlier_docs = jnp.concatenate([jnp.full((reach,), -1, dtype=jnp.int32), documents.astype(jnp.int32)])

    def convolve(pre_values, tap_rows):
        extended = jnp.pad(lax.optimization_barrier(pre_values).astype(jnp.float32), ((reach, 0), (0, 0)))
        summed = jnp.zeros((TOKENS, FF), jnp.float32)
        for shift_by in range(TAPS):
            same_doc = (earlier_docs[shift_by:shift_by + TOKENS] == documents)[:, None]
            summed = summed + jnp.where(same_doc, tap_rows[shift_by][None, :] * extended[shift_by:shift_by + TOKENS], 0.0)
        return summed
    hidden = (jax.nn.gelu(convolve(gate_pre, gate_taps), approximate=True) * convolve(value_pre, value_taps)).astype(jnp.bfloat16)
    group = FF // N_TP
    lifted = jnp.zeros((TOKENS, D), jnp.float32)
    for member in range(N_TP):
        term = lax.dot_general(hidden[:, member * group:(member + 1) * group], down_weight[:, member * group:(member + 1) * group], (((1,), (1,)), ((), ())), preferred_element_type=jnp.float32).astype(jnp.bfloat16)
        lifted = lifted + lax.optimization_barrier(term).astype(jnp.float32)
    return (stream + rms_scale(lifted, mlp_gain)).astype(jnp.bfloat16)
```

```python
import functools
import math

import jax
import jax.numpy as jnp
from jax import lax
from jax.experimental import pallas as pl
from jax.experimental.pallas import tpu as pltpu
from jax.sharding import Mesh
from jax.sharding import PartitionSpec as P


epsilon = 1e-06
masked_score = -1e30
N_Y = 4
N_CORE = 2
TP = 4
SPAN = 8192
ROWS = 256
EXTRA = 16
STATS = 16
SEQ = ("z", "y", "c")


def rms_scale(values_in, gain):
    return (
        values_in
        * lax.rsqrt(jnp.mean(values_in * values_in, axis=-1, keepdims=True) + epsilon)
        * gain
    )


def three_parts(x):
    high = x.astype(jnp.bfloat16).astype(jnp.float32)
    rest = x - high
    middle = rest.astype(jnp.bfloat16).astype(jnp.float32)
    return high, middle, rest - middle


def attend_kernel(step, last_step, factor, where_ref, q_ref, kv_ref, *refs):
    first, last = step == 0, step == last_step
    if first:
        old_acc = old_ml = None
    else:
        old_acc, old_ml = refs[:2]
        refs = refs[2:]
    if last:
        sent_ref = refs[0]
        refs = refs[1:]
    else:
        new_acc, new_ml = refs[:2]
        refs = refs[2:]
    acc, m_ref, l_ref, qx_ref, vt_ref, kcol_ref, kends = refs
    i = pl.program_id(0)
    z, y = where_ref[0], where_ref[1]
    from_y = lax.rem(y - i // 2 + N_Y, N_Y)
    q_index = z * (N_Y * N_CORE) + from_y * N_CORE + lax.rem(i, 2)
    key_plane = z - step

    @pl.when(i == 0)
    def _():
        for b in range(N_CORE):
            vt_ref[b] = jnp.transpose(
                kv_ref[b, 0:ROWS, 128:256].astype(jnp.float32)
            ).astype(jnp.bfloat16)
            docs = kv_ref[b, ROWS : ROWS + EXTRA, :].astype(jnp.float32)[0:1]
            kends[2 * b] = jnp.min(docs)
            kends[2 * b + 1] = jnp.max(docs)
            kcol_ref[b] = jnp.transpose(jnp.broadcast_to(docs, (128, ROWS)))

    if first:
        acc[...] = jnp.zeros_like(acc)
        m_ref[...] = jnp.full(m_ref.shape, masked_score, jnp.float32)
        l_ref[...] = jnp.zeros_like(l_ref)
    else:
        acc[...] = old_acc[0]
        m_ref[...] = old_ml[0, 0:1]
        l_ref[...] = old_ml[0, 1:2]

    queries = q_ref[0, 0:ROWS, :].astype(jnp.float32)
    lane = lax.broadcasted_iota(jnp.int32, (ROWS, 128), 1)
    qx_ref[0:ROWS] = jnp.where(lane < 64, queries, 0.0).astype(jnp.bfloat16)
    qx_ref[ROWS : 2 * ROWS] = jnp.where(lane < 64, 0.0, queries).astype(jnp.bfloat16)
    q_tail = q_ref[0, ROWS : ROWS + EXTRA, :].astype(jnp.float32)
    q_docs = jnp.concatenate([q_tail[0:1], q_tail[1:2], q_tail[0:1], q_tail[1:2]], axis=1)
    q_first, q_last = jnp.min(q_docs), jnp.max(q_docs)

    def update(b, k_index, masked):
        scores = lax.dot_general(
            kv_ref[b, 0:ROWS, 0:128],
            qx_ref[...],
            (((1,), (1,)), ((), ())),
            preferred_element_type=jnp.float32,
        )
        if masked:
            row = lax.broadcasted_iota(jnp.int32, (ROWS, 2 * ROWS), 0)
            col = lax.broadcasted_iota(jnp.int32, (ROWS, 2 * ROWS), 1) & (ROWS - 1)
            ahead = (k_index - q_index) * ROWS
            same = jnp.broadcast_to(kcol_ref[b][:, 0:1], (ROWS, 2 * ROWS)) == q_docs
            allowed = same & (row + ahead <= col)
            scores = jnp.where(allowed, scores, masked_score)
        old_max = m_ref[...]
        new_max = jnp.maximum(old_max, jnp.max(scores, axis=0, keepdims=True))
        probs = jnp.exp2((scores - new_max) * factor)
        if masked:
            probs = jnp.where(allowed, probs, 0.0)
        rescale = jnp.exp2((old_max - new_max) * factor)
        m_ref[...] = new_max
        l_ref[...] = l_ref[...] * rescale + jnp.sum(probs, axis=0, keepdims=True)
        acc[...] = acc[...] * rescale + jnp.dot(
            vt_ref[b], probs.astype(jnp.bfloat16), preferred_element_type=jnp.float32
        )

    for b in range(N_CORE):
        k_index = key_plane * (N_Y * N_CORE) + y * N_CORE + b
        k_first, k_last = kends[2 * b], kends[2 * b + 1]
        live = (key_plane >= 0) & (k_index <= q_index) & (k_last >= q_first)
        clean = (k_index < q_index) & (k_first == q_last)
        pl.when(live & clean)(functools.partial(update, b, k_index, False))
        pl.when(live & jnp.logical_not(clean))(functools.partial(update, b, k_index, True))

    if last:
        sent_ref[0, 0:128] = acc[...].astype(jnp.bfloat16)
        row = lax.broadcasted_iota(jnp.int32, (STATS, 2 * ROWS), 0)
        stats = jnp.zeros((STATS, 2 * ROWS), jnp.float32)
        parts = (*three_parts(m_ref[...]), *three_parts(l_ref[...]))
        for n, part in enumerate(parts):
            stats = jnp.where(row == n, jnp.broadcast_to(part, stats.shape), stats)
        sent_ref[0, 128 : 128 + STATS] = stats.astype(jnp.bfloat16)
    else:
        new_acc[0] = acc[...]
        new_ml[0, 0:1] = m_ref[...]
        new_ml[0, 1:2] = l_ref[...]


def attend(step, last_step, factor, where, q_all, kv, state):
    blocks = q_all.shape[0]
    acc_spec = pl.BlockSpec((1, 128, 2 * ROWS), lambda i, w: (i, 0, 0))
    ml_spec = pl.BlockSpec((1, 8, 2 * ROWS), lambda i, w: (i, 0, 0))
    in_specs = [
        pl.BlockSpec((1, ROWS + EXTRA, 128), lambda i, w: (i, 0, 0)),
        pl.BlockSpec((N_CORE, ROWS + EXTRA, 256), lambda i, w: (0, 0, 0)),
    ]
    if step > 0:
        in_specs += [acc_spec, ml_spec]
    if step == last_step:
        out_shape = jax.ShapeDtypeStruct((blocks, 128 + STATS, 2 * ROWS), jnp.bfloat16)
        out_specs = pl.BlockSpec((1, 128 + STATS, 2 * ROWS), lambda i, w: (i, 0, 0))
    else:
        out_shape = (
            jax.ShapeDtypeStruct((blocks, 128, 2 * ROWS), jnp.float32),
            jax.ShapeDtypeStruct((blocks, 8, 2 * ROWS), jnp.float32),
        )
        out_specs = (acc_spec, ml_spec)
    pairs = blocks * N_CORE * ROWS * 2 * ROWS
    return pl.pallas_call(
        functools.partial(attend_kernel, step, last_step, factor),
        out_shape=out_shape,
        grid_spec=pltpu.PrefetchScalarGridSpec(
            num_scalar_prefetch=1,
            grid=(blocks,),
            in_specs=in_specs,
            out_specs=out_specs,
            scratch_shapes=[
                pltpu.VMEM((128, 2 * ROWS), jnp.float32),
                pltpu.VMEM((1, 2 * ROWS), jnp.float32),
                pltpu.VMEM((1, 2 * ROWS), jnp.float32),
                pltpu.VMEM((2 * ROWS, 128), jnp.bfloat16),
                pltpu.VMEM((N_CORE, 128, ROWS), jnp.bfloat16),
                pltpu.VMEM((N_CORE, ROWS, 128), jnp.float32),
                pltpu.SMEM((2 * N_CORE,), jnp.float32),
            ],
        ),
        cost_estimate=pl.CostEstimate(
            flops=pairs * 512, transcendentals=pairs, bytes_accessed=8 << 20
        ),
        name=f"attend_{step}",
    )(where, q_all, kv, *state)


def merge_kernel(factor, lam_ref, gain_ref, *refs):
    out_ref = refs[-1]
    parts = []
    for ref in refs[:-1]:
        stats = ref[0, 128 : 128 + STATS].astype(jnp.float32)
        parts.append(
            (
                stats[0:1] + stats[1:2] + stats[2:3],
                stats[3:4] + stats[4:5] + stats[5:6],
                ref,
            )
        )
    top = functools.reduce(jnp.maximum, [m for m, _, _ in parts])
    total = jnp.zeros_like(top)
    weighted = jnp.zeros((128, 2 * ROWS), jnp.float32)
    for m, l, ref in parts:
        scale = jnp.exp2((m - top) * factor)
        total = total + l * scale
        weighted = weighted + ref[0, 0:128].astype(jnp.float32) * scale
    weighted = weighted / total
    heads = weighted[:, 0:ROWS] - lam_ref[0] * weighted[:, ROWS : 2 * ROWS]
    mean = jnp.mean(heads * heads, axis=0, keepdims=True)
    out_ref[0] = (heads * lax.rsqrt(mean + epsilon) * gain_ref[...]).astype(jnp.bfloat16)


def merge(factor, lam, gain, sources):
    spec = pl.BlockSpec((1, 128 + STATS, 2 * ROWS), lambda i: (i, 0, 0))
    return pl.pallas_call(
        functools.partial(merge_kernel, factor),
        out_shape=jax.ShapeDtypeStruct((N_CORE, 128, ROWS), jnp.bfloat16),
        grid=(N_CORE,),
        in_specs=[
            pl.BlockSpec(memory_space=pltpu.SMEM),
            pl.BlockSpec((128, 1), lambda i: (0, 0)),
            *([spec] * len(sources)),
        ],
        out_specs=pl.BlockSpec((1, 128, ROWS), lambda i: (i, 0, 0)),
        cost_estimate=pl.CostEstimate(
            flops=8 * 4 * 128 * 1024, transcendentals=1024 * 16, bytes_accessed=2 << 20
        ),
        name="merge",
    )(lam, gain, *sources)


def round_by(array, axis, by):
    length = lax.axis_size(axis)
    return lax.ppermute(array, axis, [(i, (i + by) % length) for i in range(length)])


def per_device(
    residual,
    queries,
    keys,
    values,
    documents,
    lambdas,
    head_gain,
    out_weight,
    mix_gain,
    pre_gain,
    gate_weight,
    value_weight,
    gate_taps,
    value_taps,
    down_weight,
    mlp_gain,
):
    tok_rows = residual.shape[0]
    score_scale = (queries.shape[2] // 2) ** (-0.5)
    factor = score_scale * math.log2(math.e)
    z_at, y_at, core = lax.axis_index("z"), lax.axis_index("y"), lax.axis_index("c")
    where = jnp.stack([z_at, y_at]).astype(jnp.int32)

    weights = lax.all_gather(
        jnp.concatenate([gate_weight, value_weight, down_weight], axis=1), SEQ, axis=0, tiled=True
    )

    docs = documents.astype(jnp.bfloat16)
    tail = jnp.zeros((EXTRA, 384), jnp.bfloat16)
    tail = tail.at[0, 0:128].set(docs[0:128]).at[1, 0:128].set(docs[128:256])
    tail = tail.at[0, 128:384].set(docs)
    both = jnp.concatenate(
        [
            jnp.transpose(jnp.concatenate([queries, keys, values], axis=2), (1, 0, 2)),
            jnp.broadcast_to(tail, (2, EXTRA, 384)),
        ],
        axis=1,
    )
    held = lax.all_to_all(both, "c", 0, 0, tiled=True)
    q_own, kv = held[:, :, 0:128], held[:, :, 128:384]

    planes = SPAN // (tok_rows * N_Y * N_CORE)
    q_all = jnp.concatenate([q_own, *(round_by(q_own, "y", r) for r in range(1, N_Y))], axis=0)
    state = ()
    for step in range(planes + 1):
        coming = round_by(kv, "z", 1) if step < planes else None
        state = attend(step, planes, factor, where, q_all, kv, state)
        kv = coming
    sources = [state[0:N_CORE]]
    for r in range(1, N_Y):
        sources.append(round_by(state[r * N_CORE : (r + 1) * N_CORE], "y", -r))
    lam = lax.dynamic_slice_in_dim(lambdas, core, 1)
    gain = lax.dynamic_slice_in_dim(head_gain, core, 1, 0).reshape(128, 1)
    normed = merge(factor, lam, gain, sources)

    spread = jnp.broadcast_to(normed[None], (TP, N_CORE, 128, tok_rows)).reshape(
        TP * N_CORE, 128, tok_rows
    )
    all_heads = lax.all_to_all(spread, ("tp", "c"), 0, 0, tiled=True).reshape(-1, tok_rows)
    mixed = lax.dot_general(
        all_heads, out_weight, (((0,), (0,)), ((), ())), preferred_element_type=jnp.float32
    )
    stream = residual.astype(jnp.float32) + rms_scale(mixed, mix_gain)
    normal_input = rms_scale(stream, pre_gain).astype(jnp.bfloat16)

    hidden_units = gate_weight.shape[1]
    pre = jnp.dot(
        normal_input, weights[:, 0 : 2 * hidden_units], preferred_element_type=jnp.float32
    ).astype(jnp.bfloat16)
    reach = gate_taps.shape[0] - 1
    rim = jnp.concatenate(
        [
            pre[tok_rows - reach :],
            jnp.broadcast_to(docs[tok_rows - reach :, None], (reach, 128)),
        ],
        axis=1,
    )
    length = lax.axis_size(SEQ)
    rim = lax.ppermute(rim, SEQ, [(i, i + 1) for i in range(length - 1)])
    earlier_docs = jnp.concatenate([rim[:, 2 * hidden_units].astype(jnp.int32), documents])

    taps = jnp.concatenate([gate_taps, value_taps], axis=1)
    extended = lax.optimization_barrier(
        jnp.concatenate([rim[:, 0 : 2 * hidden_units], pre])
    ).astype(jnp.float32)
    summed = jnp.zeros((tok_rows, 2 * hidden_units), jnp.float32)
    for shift_by in range(reach + 1):
        same_doc = (earlier_docs[shift_by : shift_by + tok_rows] == documents)[:, None]
        summed = summed + jnp.where(
            same_doc, taps[shift_by][None, :] * extended[shift_by : shift_by + tok_rows], 0.0
        )
    hidden = (
        jax.nn.gelu(summed[:, 0:hidden_units], approximate=True) * summed[:, hidden_units:]
    ).astype(jnp.bfloat16)
    down_terms = lax.dot_general(
        hidden,
        weights[:, 2 * hidden_units :],
        (((1,), (1,)), ((), ())),
        preferred_element_type=jnp.float32,
    ).astype(jnp.bfloat16)

    part = tok_rows // TP
    terms = lax.all_to_all(down_terms, "tp", 0, 0, tiled=True).reshape(TP, part, -1)
    lifted = jnp.sum(terms.astype(jnp.float32), axis=0)
    own_stream = lax.dynamic_slice_in_dim(stream, lax.axis_index("tp") * part, part, 0)
    out = (own_stream + rms_scale(lifted, mlp_gain)).astype(jnp.bfloat16)
    copies = jnp.broadcast_to(out[None], (TP, *out.shape)).reshape(tok_rows, -1)
    return lax.all_to_all(copies, "tp", 0, 0, tiled=True)


def solution(mesh):
    devices = mesh.devices
    split = Mesh(
        devices.reshape(devices.shape[0] // (N_Y * N_CORE), N_Y, N_CORE, devices.shape[1]),
        ("z", "y", "c", "tp"),
    )
    placed = (
        P(SEQ, None),
        P(SEQ, "tp", None),
        P(SEQ, "tp", None),
        P(SEQ, "tp", None),
        P(SEQ),
        P("tp"),
        P("tp", None),
        P(),
        P(),
        P(),
        P(SEQ, "tp"),
        P(SEQ, "tp"),
        P(None, "tp"),
        P(None, "tp"),
        P(SEQ, "tp"),
        P(),
    )
    return jax.shard_map(
        per_device, mesh=split, in_specs=placed, out_specs=P(SEQ, None), check_vma=False
    )
```

```python
import functools
import math

import jax
import jax.numpy as jnp
from jax import lax
from jax.experimental import pallas as pl
from jax.experimental.pallas import tpu as pltpu
from jax.sharding import Mesh
from jax.sharding import PartitionSpec as P


epsilon = 1e-06
masked_score = -1e30
N_Y = 4
N_CORE = 2
TP = 4
SPAN = 8192
ROWS = 256
EXTRA = 16
STATS = 16
SEQ = ("z", "y", "c")
VMEM_LIMIT = 16 << 20


def rms_scale(values_in, gain):
    return (
        values_in
        * lax.rsqrt(jnp.mean(values_in * values_in, axis=-1, keepdims=True) + epsilon)
        * gain
    )


def three_parts(x):
    high = x.astype(jnp.bfloat16).astype(jnp.float32)
    rest = x - high
    middle = rest.astype(jnp.bfloat16).astype(jnp.float32)
    return high, middle, rest - middle


def attend_kernel(step, last, factor, first_block, blocks, where_ref, q_ref, kv_ref, *refs):
    first = step == 0
    if first:
        old_acc = old_ml = None
    else:
        old_acc, old_ml = refs[:2]
        refs = refs[2:]
    if last:
        sent_ref, new_acc, new_ml = refs[:3]
        refs = refs[3:]
    else:
        new_acc, new_ml = refs[:2]
        refs = refs[2:]
    qx_ref, vt_ref, kcol_ref, ends = refs
    z, y = where_ref[0], where_ref[1]
    key_plane = z - step
    keys = N_CORE * ROWS

    for b in range(N_CORE):
        vt_ref[:, b * ROWS : (b + 1) * ROWS] = jnp.transpose(
            kv_ref[b, 0:ROWS, 128:256].astype(jnp.float32)
        ).astype(jnp.bfloat16)
        docs = kv_ref[b, ROWS : ROWS + EXTRA, :].astype(jnp.float32)[0:1]
        if b == 0:
            ends[0] = jnp.min(docs)
        if b == N_CORE - 1:
            ends[1] = jnp.max(docs)
        kcol_ref[b * ROWS : (b + 1) * ROWS] = jnp.transpose(jnp.broadcast_to(docs, (128, ROWS)))
    for n in range(blocks):
        q_tail = q_ref[first_block + n, ROWS : ROWS + EXTRA, :].astype(jnp.float32)
        ends[2 + 2 * n] = jnp.min(q_tail[0:1])
        ends[3 + 2 * n] = jnp.max(q_tail[1:2])

    @pl.loop(0, blocks)
    def _(n):
        i = n + first_block
        acc, ml = (new_acc, new_ml) if last else (new_acc.at[n], new_ml.at[n])
        from_y = lax.rem(y - i // 2 + N_Y, N_Y)
        q_index = z * (N_Y * N_CORE) + from_y * N_CORE + lax.rem(i, 2)
        k_index = key_plane * (N_Y * N_CORE) + y * N_CORE
        live = (key_plane >= 0) & (k_index <= q_index) & (ends[1] >= ends[2 + 2 * n])
        clean = (k_index + N_CORE - 1 < q_index) & (ends[0] == ends[3 + 2 * n])

        def update(masked):
            queries = q_ref[i, 0:ROWS, :].astype(jnp.float32)
            lane = lax.broadcasted_iota(jnp.int32, (ROWS, 128), 1)
            qx_ref[0:ROWS] = jnp.where(lane < 64, queries, 0.0).astype(jnp.bfloat16)
            qx_ref[ROWS : 2 * ROWS] = jnp.where(lane < 64, 0.0, queries).astype(jnp.bfloat16)
            key_rows = kv_ref[:, 0:ROWS, 0:128].reshape(keys, 128)
            if masked:
                q_tail = q_ref[i, ROWS : ROWS + EXTRA, :].astype(jnp.float32)
                q_docs = jnp.concatenate([q_tail[0:1], q_tail[1:2]], axis=1)
                row = lax.broadcasted_iota(jnp.int32, (keys, ROWS), 0)
                col = lax.broadcasted_iota(jnp.int32, (keys, ROWS), 1)
                ahead = (k_index - q_index) * ROWS
                same = jnp.broadcast_to(kcol_ref[:, 0:1], (keys, ROWS)) == q_docs
                allowed = same & (row + ahead <= col)
            all_scores = [
                lax.dot_general(
                    key_rows,
                    qx_ref[m * ROWS : (m + 1) * ROWS],
                    (((1,), (1,)), ((), ())),
                    preferred_element_type=jnp.float32,
                )
                for m in range(2)
            ]
            for m, scores in enumerate(all_scores):
                span = slice(m * ROWS, (m + 1) * ROWS)
                if masked:
                    scores = jnp.where(allowed, scores, masked_score)
                new_max = jnp.max(scores, axis=0, keepdims=True)
                if not first:
                    old_max = old_ml[i, 0:1, span]
                    new_max = jnp.maximum(old_max, new_max)
                    rescale = jnp.exp2((old_max - new_max) * factor)
                probs = jnp.exp2((scores - new_max) * factor)
                if masked:
                    probs = jnp.where(allowed, probs, 0.0)
                total = jnp.sum(probs, axis=0, keepdims=True)
                weighted = jnp.dot(
                    vt_ref[...], probs.astype(jnp.bfloat16), preferred_element_type=jnp.float32
                )
                if not first:
                    total = total + old_ml[i, 1:2, span] * rescale
                    weighted = weighted + old_acc[i, :, span] * rescale
                ml[0:1, span] = new_max
                ml[1:2, span] = total
                acc[:, span] = weighted

        pl.when(live & clean)(functools.partial(update, False))
        pl.when(live & jnp.logical_not(clean))(functools.partial(update, True))

        @pl.when(jnp.logical_not(live))
        def _():
            if first:
                acc[...] = jnp.zeros(acc.shape, jnp.float32)
                ml[0:1] = jnp.full((1, 2 * ROWS), masked_score, jnp.float32)
                ml[1:2] = jnp.zeros((1, 2 * ROWS), jnp.float32)
            else:
                acc[...] = old_acc[i]
                ml[0:2] = old_ml[i, 0:2]

        if last:
            sent_ref[n, 0:128] = acc[...].astype(jnp.bfloat16)
            row = lax.broadcasted_iota(jnp.int32, (STATS, 2 * ROWS), 0)
            stats = jnp.zeros((STATS, 2 * ROWS), jnp.float32)
            parts = (*three_parts(ml[0:1]), *three_parts(ml[1:2]))
            for j, part in enumerate(parts):
                stats = jnp.where(row == j, jnp.broadcast_to(part, stats.shape), stats)
            sent_ref[n, 128 : 128 + STATS] = stats.astype(jnp.bfloat16)


def attend(step, last, factor, where, q_all, kv, state, first_block=0, blocks=None):
    blocks = q_all.shape[0] if blocks is None else blocks
    acc_block, ml_block = (128, 2 * ROWS), (8, 2 * ROWS)
    vmem = pl.BlockSpec(memory_space=pltpu.VMEM)
    in_specs = [pl.BlockSpec(memory_space=pltpu.SMEM)] + [vmem] * (2 + len(state))
    scratch = [
        pltpu.VMEM((2 * ROWS, 128), jnp.bfloat16),
        pltpu.VMEM((128, N_CORE * ROWS), jnp.bfloat16),
        pltpu.VMEM((N_CORE * ROWS, 128), jnp.float32),
        pltpu.SMEM((2 + 2 * blocks,), jnp.float32),
    ]
    aliases = {}
    if last:
        out_shape = jax.ShapeDtypeStruct((blocks, 128 + STATS, 2 * ROWS), jnp.bfloat16)
        out_specs = vmem
        scratch = [pltpu.VMEM(acc_block, jnp.float32), pltpu.VMEM(ml_block, jnp.float32)] + scratch
    else:
        out_shape = (
            jax.ShapeDtypeStruct((blocks, *acc_block), jnp.float32),
            jax.ShapeDtypeStruct((blocks, *ml_block), jnp.float32),
        )
        out_specs = (vmem, vmem)
        if step > 0:
            aliases = {3: 0, 4: 1}
    pairs = blocks * N_CORE * ROWS * 2 * ROWS
    return pl.pallas_call(
        functools.partial(attend_kernel, step, last, factor, first_block, blocks),
        out_shape=out_shape,
        in_specs=in_specs,
        out_specs=out_specs,
        scratch_shapes=scratch,
        input_output_aliases=aliases,
        compiler_params=pltpu.CompilerParams(vmem_limit_bytes=VMEM_LIMIT),
        cost_estimate=pl.CostEstimate(
            flops=pairs * 512, transcendentals=pairs, bytes_accessed=blocks << 20
        ),
        name=f"attend_{step}_{first_block}",
    )(where, q_all, kv, *state)


def merge_kernel(factor, where_ref, lam_ref, gain_ref, *refs):
    out_ref = refs[-1]
    core = where_ref[2]
    gains = jnp.where(core == 0, gain_ref[0:1], gain_ref[1:2])
    gain = jnp.transpose(jnp.broadcast_to(gains, (128, 128)))[:, 0:1]
    lam = jnp.where(core == 0, lam_ref[0], lam_ref[1])
    for half in range(N_CORE):
        parts = []
        for ref in refs[:-1]:
            stats = ref[half, 128 : 128 + STATS].astype(jnp.float32)
            parts.append(
                (
                    stats[0:1] + stats[1:2] + stats[2:3],
                    stats[3:4] + stats[4:5] + stats[5:6],
                    ref,
                )
            )
        top = functools.reduce(jnp.maximum, [m for m, _, _ in parts])
        total = jnp.zeros_like(top)
        weighted = jnp.zeros((128, 2 * ROWS), jnp.float32)
        for m, l, ref in parts:
            scale = jnp.exp2((m - top) * factor)
            total = total + l * scale
            weighted = weighted + ref[half, 0:128].astype(jnp.float32) * scale
        weighted = weighted / total
        heads = weighted[:, 0:ROWS] - lam * weighted[:, ROWS : 2 * ROWS]
        mean = jnp.mean(heads * heads, axis=0, keepdims=True)
        normed = (heads * lax.rsqrt(mean + epsilon) * gain).astype(jnp.bfloat16)
        for t in range(TP):
            out_ref[t * N_CORE + half] = normed


def merge(factor, where, lam, gain, sources):
    smem, vmem = (pl.BlockSpec(memory_space=m) for m in (pltpu.SMEM, pltpu.VMEM))
    return pl.pallas_call(
        functools.partial(merge_kernel, factor),
        out_shape=jax.ShapeDtypeStruct((TP * N_CORE, 128, ROWS), jnp.bfloat16),
        in_specs=[smem, smem, vmem, *([vmem] * len(sources))],
        out_specs=vmem,
        compiler_params=pltpu.CompilerParams(vmem_limit_bytes=VMEM_LIMIT),
        cost_estimate=pl.CostEstimate(
            flops=8 * 4 * 128 * 1024, transcendentals=1024 * 16, bytes_accessed=2 << 20
        ),
        name="merge",
    )(where, lam, gain, *sources)


def round_by(array, axis, by):
    length = lax.axis_size(axis)
    return lax.ppermute(array, axis, [(i, (i + by) % length) for i in range(length)])


def per_device(
    residual,
    queries,
    keys,
    values,
    documents,
    lambdas,
    head_gain,
    out_weight,
    mix_gain,
    pre_gain,
    gate_weight,
    value_weight,
    gate_taps,
    value_taps,
    down_weight,
    mlp_gain,
):
    tok_rows = residual.shape[0]
    score_scale = (queries.shape[2] // 2) ** (-0.5)
    factor = score_scale * math.log2(math.e)
    z_at, y_at, core = lax.axis_index("z"), lax.axis_index("y"), lax.axis_index("c")
    where = jnp.stack([z_at, y_at, core]).astype(jnp.int32)

    docs = documents.astype(jnp.bfloat16)
    doc_rows = docs.reshape(2, 128)
    tail = jnp.concatenate(
        [
            jnp.concatenate([doc_rows, jnp.zeros((EXTRA - 2, 128), jnp.bfloat16)], axis=0),
            jnp.broadcast_to(docs[None, :], (EXTRA, 256)),
        ],
        axis=1,
    )
    both = jnp.concatenate(
        [
            jnp.transpose(jnp.concatenate([queries, keys, values], axis=2), (1, 0, 2)),
            jnp.broadcast_to(tail, (2, EXTRA, 384)),
        ],
        axis=1,
    )
    held = lax.all_to_all(both, "c", 0, 0, tiled=True)
    q_own, kv = held[:, :, 0:128], held[:, :, 128:384]
    weights = lax.all_gather(
        jnp.concatenate([gate_weight, value_weight, down_weight], axis=1), SEQ, axis=0, tiled=True
    )

    planes = SPAN // (tok_rows * N_Y * N_CORE)
    q_all = jnp.concatenate([q_own, *(round_by(q_own, "y", r) for r in range(1, N_Y))], axis=0)
    state = ()
    for step in range(planes):
        if step > 1:
            kv, done = lax.optimization_barrier((kv, older))
        coming = round_by(kv, "z", 1)
        older = state
        state = attend(step, False, factor, where, q_all, kv, state)
        kv = coming
    sources = [None] * N_Y
    for r in (2, 1, 3, 0):
        sent = attend(planes, True, factor, where, q_all, kv, state, r * N_CORE, N_CORE)
        sources[r] = round_by(sent, "y", -r) if r else sent
    spread = merge(factor, where, lambdas, head_gain, sources)
    all_heads = lax.all_to_all(spread, ("tp", "c"), 0, 0, tiled=True).reshape(-1, tok_rows)
    mixed = lax.dot_general(
        all_heads, out_weight, (((0,), (0,)), ((), ())), preferred_element_type=jnp.float32
    )
    stream = residual.astype(jnp.float32) + rms_scale(mixed, mix_gain)
    normal_input = rms_scale(stream, pre_gain).astype(jnp.bfloat16)

    hidden_units = gate_weight.shape[1]
    pre = jnp.dot(
        normal_input, weights[:, 0 : 2 * hidden_units], preferred_element_type=jnp.float32
    ).astype(jnp.bfloat16)
    reach = gate_taps.shape[0] - 1
    rim = jnp.concatenate(
        [
            pre[tok_rows - reach :],
            jnp.broadcast_to(docs[tok_rows - reach :, None], (reach, 128)),
        ],
        axis=1,
    )
    length = lax.axis_size(SEQ)
    rim = lax.ppermute(rim, SEQ, [(i, i + 1) for i in range(length - 1)])
    earlier_docs = jnp.concatenate([rim[:, 2 * hidden_units].astype(jnp.int32), documents])

    taps = jnp.concatenate([gate_taps, value_taps], axis=1)
    extended = lax.optimization_barrier(
        jnp.concatenate([rim[:, 0 : 2 * hidden_units], pre])
    ).astype(jnp.float32)
    summed = jnp.zeros((tok_rows, 2 * hidden_units), jnp.float32)
    for shift_by in range(reach + 1):
        same_doc = (earlier_docs[shift_by : shift_by + tok_rows] == documents)[:, None]
        summed = summed + jnp.where(
            same_doc, taps[shift_by][None, :] * extended[shift_by : shift_by + tok_rows], 0.0
        )
    hidden = (
        jax.nn.gelu(summed[:, 0:hidden_units], approximate=True) * summed[:, hidden_units:]
    ).astype(jnp.bfloat16)
    down_terms = lax.dot_general(
        hidden,
        weights[:, 2 * hidden_units :],
        (((1,), (1,)), ((), ())),
        preferred_element_type=jnp.float32,
    ).astype(jnp.bfloat16)

    part = tok_rows // TP
    terms = lax.all_to_all(down_terms, "tp", 0, 0, tiled=True).reshape(TP, part, -1)
    lifted = jnp.sum(terms.astype(jnp.float32), axis=0)
    own_stream = lax.dynamic_slice_in_dim(stream, lax.axis_index("tp") * part, part, 0)
    out = (own_stream + rms_scale(lifted, mlp_gain)).astype(jnp.bfloat16)
    copies = jnp.broadcast_to(out[None], (TP, *out.shape)).reshape(tok_rows, -1)
    return lax.all_to_all(copies, "tp", 0, 0, tiled=True)


def solution(mesh):
    devices = mesh.devices
    split = Mesh(
        devices.reshape(devices.shape[0] // (N_Y * N_CORE), N_Y, N_CORE, devices.shape[1]),
        ("z", "y", "c", "tp"),
    )
    placed = (
        P(SEQ, None),
        P(SEQ, "tp", None),
        P(SEQ, "tp", None),
        P(SEQ, "tp", None),
        P(SEQ),
        P("tp"),
        P("tp", None),
        P(),
        P(),
        P(),
        P(SEQ, "tp"),
        P(SEQ, "tp"),
        P(None, "tp"),
        P(None, "tp"),
        P(SEQ, "tp"),
        P(),
    )
    return jax.shard_map(
        per_device, mesh=split, in_specs=placed, out_specs=P(SEQ, None), check_vma=False
    )
```

```python
import functools
import math

import jax
import jax.numpy as jnp
from jax import lax
from jax.experimental import pallas as pl
from jax.experimental.pallas import tpu as pltpu
from jax.sharding import Mesh
from jax.sharding import PartitionSpec as P


epsilon = 1e-06
masked_score = -1e30
N_Y = 4
N_CORE = 2
TP = 4
SPAN = 8192
ROWS = 256
EXTRA = 16
SEQ = ("z", "y", "c")
VMEM_LIMIT = 16 << 20


def rms_scale(values_in, gain):
    return (
        values_in
        * lax.rsqrt(jnp.mean(values_in * values_in, axis=-1, keepdims=True) + epsilon)
        * gain
    )


def attend_kernel(first, step, factor, where_ref, q_ref, kv_ref, *refs):
    if first:
        old_acc = old_ml = None
    else:
        old_acc, old_ml = refs[:2]
        refs = refs[2:]
    new_acc, new_ml, qx_ref, vt_ref, kcol_ref, ends = refs
    blocks = new_acc.shape[0]
    z, y = where_ref[0], where_ref[1]
    key_plane = z - step
    keys = N_CORE * ROWS

    for b in range(N_CORE):
        for half in range(2):
            at = b * ROWS + half * 128
            vt_ref[:, at : at + 128] = kv_ref[b, half * 128 : half * 128 + 128, 128:256]
    tails = [kv_ref[b, ROWS : ROWS + EXTRA, 0:128].astype(jnp.float32) for b in range(N_CORE)]
    ends[0] = jnp.min(tails[0][0:1])
    ends[1] = jnp.max(tails[N_CORE - 1][1:2])
    for n in range(blocks):
        q_tail = q_ref[n, ROWS : ROWS + EXTRA, :].astype(jnp.float32)
        ends[2 + 2 * n] = jnp.min(q_tail[0:1])
        ends[3 + 2 * n] = jnp.max(q_tail[1:2])

    @pl.loop(0, blocks)
    def _(n):
        acc = new_acc.at[n]
        this = pl.ds(n, 1)
        from_y = lax.rem(y - n // 2 + N_Y, N_Y)
        q_index = z * (N_Y * N_CORE) + from_y * N_CORE + lax.rem(n, 2)
        k_index = key_plane * (N_Y * N_CORE) + y * N_CORE
        live = (key_plane >= 0) & (k_index <= q_index) & (ends[1] >= ends[2 + 2 * n])
        clean = (k_index + N_CORE - 1 < q_index) & (ends[0] == ends[3 + 2 * n])

        def update(masked):
            queries = q_ref[n, 0:ROWS, :].astype(jnp.float32)
            lane = lax.broadcasted_iota(jnp.int32, (ROWS, 128), 1)
            qx_ref[0:ROWS] = jnp.where(lane < 64, queries, 0.0).astype(jnp.bfloat16)
            qx_ref[ROWS : 2 * ROWS] = jnp.where(lane < 64, 0.0, queries).astype(jnp.bfloat16)
            key_rows = kv_ref[:, 0:ROWS, 0:128].reshape(keys, 128)
            if masked:
                for b in range(N_CORE):
                    docs = kv_ref[b, ROWS : ROWS + EXTRA, 0:128].astype(jnp.float32)
                    for half in range(2):
                        at = b * ROWS + half * 128
                        kcol_ref[at : at + 128] = jnp.transpose(
                            jnp.broadcast_to(docs[half : half + 1], (128, 128))
                        )
                q_tail = q_ref[n, ROWS : ROWS + EXTRA, :].astype(jnp.float32)
                q_docs = jnp.concatenate([q_tail[0:1], q_tail[1:2]], axis=1)
                row = lax.broadcasted_iota(jnp.int32, (keys, ROWS), 0)
                col = lax.broadcasted_iota(jnp.int32, (keys, ROWS), 1)
                ahead = (k_index - q_index) * ROWS
                same = jnp.broadcast_to(kcol_ref[:, 0:1], (keys, ROWS)) == q_docs
                allowed = same & (row + ahead <= col)
            all_scores = [
                lax.dot_general(
                    key_rows,
                    qx_ref[m * ROWS : (m + 1) * ROWS],
                    (((1,), (1,)), ((), ())),
                    preferred_element_type=jnp.float32,
                )
                for m in range(2)
            ]
            for m, scores in enumerate(all_scores):
                span = slice(m * ROWS, (m + 1) * ROWS)
                if masked:
                    scores = jnp.where(allowed, scores, masked_score)
                new_max = jnp.max(scores, axis=0, keepdims=True)
                if not first:
                    old_max = old_ml[0, this, span]
                    new_max = jnp.maximum(old_max, new_max)
                    rescale = jnp.exp2((old_max - new_max) * factor)
                probs = jnp.exp2((scores - new_max) * factor)
                if masked:
                    probs = jnp.where(allowed, probs, 0.0)
                total = jnp.sum(probs, axis=0, keepdims=True)
                weighted = jnp.dot(
                    vt_ref[...], probs.astype(jnp.bfloat16), preferred_element_type=jnp.float32
                )
                if not first:
                    total = total + old_ml[1, this, span] * rescale
                    weighted = weighted + old_acc[n, :, span] * rescale
                new_ml[0, this, span] = new_max
                new_ml[1, this, span] = total
                acc[:, span] = weighted

        pl.when(live & clean)(functools.partial(update, False))
        pl.when(live & jnp.logical_not(clean))(functools.partial(update, True))

        @pl.when(jnp.logical_not(live))
        def _():
            if first:
                acc[...] = jnp.zeros(acc.shape, jnp.float32)
                new_ml[0, this] = jnp.full((1, 2 * ROWS), masked_score, jnp.float32)
                new_ml[1, this] = jnp.zeros((1, 2 * ROWS), jnp.float32)
            else:
                acc[...] = old_acc[n]
                new_ml[0, this] = old_ml[0, this]
                new_ml[1, this] = old_ml[1, this]


def attend(step, factor, where, q_all, kv, state):
    blocks = q_all.shape[0]
    vmem = pl.BlockSpec(memory_space=pltpu.VMEM)
    pairs = blocks * N_CORE * ROWS * 2 * ROWS
    return pl.pallas_call(
        functools.partial(attend_kernel, not state, step, factor),
        out_shape=(
            jax.ShapeDtypeStruct((blocks, 128, 2 * ROWS), jnp.float32),
            jax.ShapeDtypeStruct((2, blocks, 2 * ROWS), jnp.float32),
        ),
        in_specs=[pl.BlockSpec(memory_space=pltpu.SMEM)] + [vmem] * (2 + len(state)),
        out_specs=(vmem, vmem),
        scratch_shapes=[
            pltpu.VMEM((2 * ROWS, 128), jnp.bfloat16),
            pltpu.VMEM((128, N_CORE * ROWS), jnp.bfloat16),
            pltpu.VMEM((N_CORE * ROWS, 128), jnp.float32),
            pltpu.SMEM((2 + 2 * blocks,), jnp.float32),
        ],
        input_output_aliases={3: 0, 4: 1} if state else {},
        compiler_params=pltpu.CompilerParams(vmem_limit_bytes=VMEM_LIMIT),
        cost_estimate=pl.CostEstimate(
            flops=pairs * 512, transcendentals=pairs, bytes_accessed=blocks << 20
        ),
        name=f"attend_{step}",
    )(where, q_all, kv, *state)


def combine_kernel(factor, where_ref, lam_ref, acc_ref, ml_ref, *refs):
    others, outs = refs[: N_Y - 1], refs[N_Y - 1 :]
    blocks = acc_ref.shape[0]
    lam = jnp.where(where_ref[2] == 0, lam_ref[0], lam_ref[1])
    m_own = ml_ref[0]
    all_m, all_l = [m_own], [ml_ref[1]]
    for d, ref in enumerate(others, 1):
        shift = blocks - N_CORE * d
        all_m.append(pltpu.roll(ref[0], shift, 0))
        all_l.append(pltpu.roll(ref[1], shift, 0))
    top = functools.reduce(jnp.maximum, all_m)
    total = jnp.zeros_like(top)
    for m, l in zip(all_m, all_l):
        total = total + l * jnp.exp2((m - top) * factor)
    scale = jnp.exp2((m_own - top) * factor) / total
    lane = lax.broadcasted_iota(jnp.int32, scale.shape, 1)
    scale = jnp.where(lane < ROWS, scale, -lam * scale)
    for n in range(blocks):
        part = (
            acc_ref[n, :, 0:ROWS] * scale[n : n + 1, 0:ROWS]
            + acc_ref[n, :, ROWS : 2 * ROWS] * scale[n : n + 1, ROWS : 2 * ROWS]
        )
        outs[n // N_CORE][n % N_CORE] = part.astype(jnp.bfloat16)


def combine(factor, where, lam, acc, ml, others):
    smem, vmem = (pl.BlockSpec(memory_space=m) for m in (pltpu.SMEM, pltpu.VMEM))
    return pl.pallas_call(
        functools.partial(combine_kernel, factor),
        out_shape=[jax.ShapeDtypeStruct((N_CORE, 128, ROWS), jnp.bfloat16)] * N_Y,
        in_specs=[smem, smem, *([vmem] * (2 + len(others)))],
        out_specs=[vmem] * N_Y,
        compiler_params=pltpu.CompilerParams(vmem_limit_bytes=VMEM_LIMIT),
        cost_estimate=pl.CostEstimate(
            flops=8 * 128 * 4096, transcendentals=4096 * 5, bytes_accessed=3 << 20
        ),
        name="combine",
    )(where, lam, acc, ml, *others)


def merge_kernel(where_ref, gain_ref, *refs):
    out_ref = refs[-1]
    gains = jnp.where(where_ref[2] == 0, gain_ref[0:1], gain_ref[1:2])
    gain = jnp.transpose(jnp.broadcast_to(gains, (128, 128)))[:, 0:1]
    for half in range(N_CORE):
        heads = functools.reduce(jnp.add, [ref[half].astype(jnp.float32) for ref in refs[:-1]])
        mean = jnp.mean(heads * heads, axis=0, keepdims=True)
        normed = (heads * lax.rsqrt(mean + epsilon) * gain).astype(jnp.bfloat16)
        for t in range(TP):
            out_ref[t * N_CORE + half] = normed


def merge(where, gain, sources):
    smem, vmem = (pl.BlockSpec(memory_space=m) for m in (pltpu.SMEM, pltpu.VMEM))
    return pl.pallas_call(
        merge_kernel,
        out_shape=jax.ShapeDtypeStruct((TP * N_CORE, 128, ROWS), jnp.bfloat16),
        in_specs=[smem, vmem, *([vmem] * len(sources))],
        out_specs=vmem,
        compiler_params=pltpu.CompilerParams(vmem_limit_bytes=VMEM_LIMIT),
        cost_estimate=pl.CostEstimate(
            flops=8 * 128 * 1024, transcendentals=1024, bytes_accessed=1 << 20
        ),
        name="merge",
    )(where, gain, *sources)


def round_by(array, axis, by):
    length = lax.axis_size(axis)
    return lax.ppermute(array, axis, [(i, (i + by) % length) for i in range(length)])


def per_device(
    residual,
    queries,
    keys,
    values,
    documents,
    lambdas,
    head_gain,
    out_weight,
    mix_gain,
    pre_gain,
    gate_weight,
    value_weight,
    gate_taps,
    value_taps,
    down_weight,
    mlp_gain,
):
    tok_rows = residual.shape[0]
    score_scale = (queries.shape[2] // 2) ** (-0.5)
    factor = score_scale * math.log2(math.e)
    z_at, y_at, core = lax.axis_index("z"), lax.axis_index("y"), lax.axis_index("c")
    where = jnp.stack([z_at, y_at, core]).astype(jnp.int32)

    doc_rows = documents.reshape(2, 128).astype(jnp.bfloat16)
    tail = jnp.pad(
        jnp.concatenate([doc_rows, doc_rows], axis=1), ((0, EXTRA - 2), (0, 128))
    )
    values_across = jnp.transpose(
        values.reshape(2, 128, N_CORE, 128), (2, 0, 3, 1)
    ).reshape(N_CORE, tok_rows, 128)
    rows = [jnp.transpose(a, (1, 0, 2)) for a in (queries, keys)] + [values_across]
    both = jnp.concatenate(
        [jnp.concatenate(rows, axis=2), jnp.broadcast_to(tail, (N_CORE, EXTRA, 384))], axis=1
    )
    held = lax.all_to_all(both, "c", 0, 0, tiled=True)
    q_own, kv = held[:, :, 0:128], held[:, :, 128:384]
    weights = lax.all_gather(
        jnp.concatenate([gate_weight, value_weight, down_weight], axis=1), SEQ, axis=0, tiled=True
    )

    planes = SPAN // (tok_rows * N_Y * N_CORE)
    q_all = jnp.concatenate([q_own, *(round_by(q_own, "y", r) for r in range(1, N_Y))], axis=0)
    state = ()
    older = None
    for step in range(planes + 1):
        if step < planes:
            if step > 1:
                kv, _ = lax.optimization_barrier((kv, older))
            coming = round_by(kv, "z", 1)
        older = state
        state = attend(step, factor, where, q_all, kv, state)
        kv = coming
    acc, ml = state
    others = [round_by(ml, "y", -d) for d in range(1, N_Y)]
    parts = combine(factor, where, lambdas, acc, ml, others)
    sources = [parts[0], *(round_by(parts[r], "y", -r) for r in (2, 1, 3))]
    spread = merge(where, head_gain, sources)
    all_heads = lax.all_to_all(spread, ("tp", "c"), 0, 0, tiled=True).reshape(-1, tok_rows)
    mixed = lax.dot_general(
        all_heads, out_weight, (((0,), (0,)), ((), ())), preferred_element_type=jnp.float32
    )
    stream = residual.astype(jnp.float32) + rms_scale(mixed, mix_gain)
    normal_input = rms_scale(stream, pre_gain).astype(jnp.bfloat16)

    hidden_units = gate_weight.shape[1]
    pre = jnp.dot(
        normal_input, weights[:, 0 : 2 * hidden_units], preferred_element_type=jnp.float32
    ).astype(jnp.bfloat16)
    reach = gate_taps.shape[0] - 1
    rim = jnp.concatenate(
        [
            pre[tok_rows - reach :],
            jnp.broadcast_to(doc_rows[1, 128 - reach :, None], (reach, 128)),
        ],
        axis=1,
    )
    length = lax.axis_size(SEQ)
    rim = lax.ppermute(rim, SEQ, [(i, i + 1) for i in range(length - 1)])
    earlier_docs = jnp.concatenate([rim[:, 2 * hidden_units].astype(jnp.int32), documents])

    taps = jnp.concatenate([gate_taps, value_taps], axis=1)
    extended = lax.optimization_barrier(
        jnp.concatenate([rim[:, 0 : 2 * hidden_units], pre])
    ).astype(jnp.float32)
    summed = jnp.zeros((tok_rows, 2 * hidden_units), jnp.float32)
    for shift_by in range(reach + 1):
        same_doc = (earlier_docs[shift_by : shift_by + tok_rows] == documents)[:, None]
        summed = summed + jnp.where(
            same_doc, taps[shift_by][None, :] * extended[shift_by : shift_by + tok_rows], 0.0
        )
    hidden = (
        jax.nn.gelu(summed[:, 0:hidden_units], approximate=True) * summed[:, hidden_units:]
    ).astype(jnp.bfloat16)
    down_terms = lax.dot_general(
        hidden,
        weights[:, 2 * hidden_units :],
        (((1,), (1,)), ((), ())),
        preferred_element_type=jnp.float32,
    ).astype(jnp.bfloat16)

    part = tok_rows // TP
    terms = lax.all_to_all(down_terms, "tp", 0, 0, tiled=True).reshape(TP, part, -1)
    lifted = jnp.sum(terms.astype(jnp.float32), axis=0)
    own_stream = lax.dynamic_slice_in_dim(stream, lax.axis_index("tp") * part, part, 0)
    out = (own_stream + rms_scale(lifted, mlp_gain)).astype(jnp.bfloat16)
    copies = jnp.broadcast_to(out[None], (TP, *out.shape)).reshape(tok_rows, -1)
    return lax.all_to_all(copies, "tp", 0, 0, tiled=True)


def solution(mesh):
    devices = mesh.devices
    split = Mesh(
        devices.reshape(devices.shape[0] // (N_Y * N_CORE), N_Y, N_CORE, devices.shape[1]),
        ("z", "y", "c", "tp"),
    )
    placed = (
        P(SEQ, None),
        P(SEQ, "tp", None),
        P(SEQ, "tp", None),
        P(SEQ, "tp", None),
        P(SEQ),
        P("tp"),
        P("tp", None),
        P(),
        P(),
        P(),
        P(SEQ, "tp"),
        P(SEQ, "tp"),
        P(None, "tp"),
        P(None, "tp"),
        P(SEQ, "tp"),
        P(),
    )
    return jax.shard_map(
        per_device, mesh=split, in_specs=placed, out_specs=P(SEQ, None), check_vma=False
    )
```

```python
import functools
import math

import jax
import jax.numpy as jnp
from jax import lax
from jax.experimental import pallas as pl
from jax.experimental.pallas import tpu as pltpu
from jax.sharding import Mesh
from jax.sharding import PartitionSpec as P


epsilon = 1e-06
masked_score = -1e30
N_Y = 4
N_CORE = 2
TP = 4
SPAN = 8192
ROWS = 256
EXTRA = 16
SEQ = ("z", "y", "c")
VMEM_LIMIT = 16 << 20


def rms_scale(values_in, gain):
    return (
        values_in
        * lax.rsqrt(jnp.mean(values_in * values_in, axis=-1, keepdims=True) + epsilon)
        * gain
    )


def attend_kernel(first, step, factor, where_ref, q_ref, kv_ref, *refs):
    if first:
        old_acc = old_ml = None
    else:
        old_acc, old_ml = refs[:2]
        refs = refs[2:]
    new_acc, new_ml, qx_ref, vt_ref, kcol_ref, ends = refs
    blocks = new_acc.shape[0]
    z, y = where_ref[0], where_ref[1]
    key_plane = z - step
    keys = N_CORE * ROWS

    for b in range(N_CORE):
        for half in range(2):
            at = b * ROWS + half * 128
            vt_ref[:, at : at + 128] = kv_ref[b, half * 128 : half * 128 + 128, 128:256]
    tails = [kv_ref[b, ROWS : ROWS + EXTRA, 0:128].astype(jnp.float32) for b in range(N_CORE)]
    ends[0] = jnp.min(tails[0][0:1])
    ends[1] = jnp.max(tails[N_CORE - 1][1:2])
    for n in range(blocks):
        q_tail = q_ref[n, ROWS : ROWS + EXTRA, :].astype(jnp.float32)
        ends[2 + 2 * n] = jnp.min(q_tail[0:1])
        ends[3 + 2 * n] = jnp.max(q_tail[1:2])

    @pl.loop(0, N_Y)
    def _(r):
        from_y = lax.rem(y - r + N_Y, N_Y)
        q_index = (z * N_Y + from_y) * N_CORE
        k_index = (key_plane * N_Y + y) * N_CORE
        n0 = r * N_CORE
        q_first, q_last = ends[2 + 2 * n0], ends[1 + 2 * (n0 + N_CORE)]
        live = (key_plane >= 0) & (k_index <= q_index) & (ends[1] >= q_first)
        clean = (k_index < q_index) & (ends[0] == q_last)

        def update(masked):
            lane = lax.broadcasted_iota(jnp.int32, (ROWS, 128), 1)
            for h in range(N_CORE):
                queries = q_ref[n0 + h, 0:ROWS, :].astype(jnp.float32)
                at = h * 2 * ROWS
                qx_ref[at : at + ROWS] = jnp.where(lane < 64, queries, 0.0).astype(jnp.bfloat16)
                qx_ref[at + ROWS : at + 2 * ROWS] = jnp.where(lane < 64, 0.0, queries).astype(
                    jnp.bfloat16
                )
            key_rows = kv_ref[:, 0:ROWS, 0:128].reshape(keys, 128)
            if masked:
                for b in range(N_CORE):
                    docs = kv_ref[b, ROWS : ROWS + EXTRA, 0:128].astype(jnp.float32)
                    for half in range(2):
                        at = b * ROWS + half * 128
                        kcol_ref[at : at + 128] = jnp.transpose(
                            jnp.broadcast_to(docs[half : half + 1], (128, 128))
                        )
                row = lax.broadcasted_iota(jnp.int32, (keys, ROWS), 0)
                col = lax.broadcasted_iota(jnp.int32, (keys, ROWS), 1)
                key_docs = jnp.broadcast_to(kcol_ref[:, 0:1], (keys, ROWS))
            scores_of = [None] * (2 * N_CORE)

            def start(c):
                scores_of[c] = lax.dot_general(
                    key_rows,
                    qx_ref[c * ROWS : (c + 1) * ROWS],
                    (((1,), (1,)), ((), ())),
                    preferred_element_type=jnp.float32,
                )

            start(0)
            for c in range(2 * N_CORE):
                n, m = n0 + c // 2, c % 2
                this = pl.ds(n, 1)
                span = slice(m * ROWS, (m + 1) * ROWS)
                if c + 1 < 2 * N_CORE:
                    start(c + 1)
                scores = scores_of[c]
                if masked:
                    if m == 0:
                        q_tail = q_ref[n, ROWS : ROWS + EXTRA, :].astype(jnp.float32)
                        q_docs = jnp.concatenate([q_tail[0:1], q_tail[1:2]], axis=1)
                        ahead = (k_index - q_index - c // 2) * ROWS
                        allowed = (key_docs == q_docs) & (row + ahead <= col)
                    scores = jnp.where(allowed, scores, masked_score)
                new_max = jnp.max(scores, axis=0, keepdims=True)
                if not first:
                    old_max = old_ml[0, this, span]
                    new_max = jnp.maximum(old_max, new_max)
                    rescale = jnp.exp2((old_max - new_max) * factor)
                probs = jnp.exp2((scores - new_max) * factor)
                if masked:
                    probs = jnp.where(allowed, probs, 0.0)
                total = jnp.sum(probs, axis=0, keepdims=True)
                weighted = jnp.dot(
                    vt_ref[...], probs.astype(jnp.bfloat16), preferred_element_type=jnp.float32
                )
                if not first:
                    total = total + old_ml[1, this, span] * rescale
                    weighted = weighted + old_acc[n, :, span] * rescale
                new_ml[0, this, span] = new_max
                new_ml[1, this, span] = total
                new_acc[n, :, span] = weighted

        pl.when(live & clean)(functools.partial(update, False))
        pl.when(live & jnp.logical_not(clean))(functools.partial(update, True))

        @pl.when(jnp.logical_not(live))
        def _():
            for h in range(N_CORE):
                n = n0 + h
                this = pl.ds(n, 1)
                if first:
                    new_acc[n] = jnp.zeros(new_acc.shape[1:], jnp.float32)
                    new_ml[0, this] = jnp.full((1, 2 * ROWS), masked_score, jnp.float32)
                    new_ml[1, this] = jnp.zeros((1, 2 * ROWS), jnp.float32)
                else:
                    new_acc[n] = old_acc[n]
                    new_ml[0, this] = old_ml[0, this]
                    new_ml[1, this] = old_ml[1, this]


def attend(step, factor, where, q_all, kv, state):
    blocks = q_all.shape[0]
    vmem = pl.BlockSpec(memory_space=pltpu.VMEM)
    pairs = blocks * N_CORE * ROWS * 2 * ROWS
    return pl.pallas_call(
        functools.partial(attend_kernel, not state, step, factor),
        out_shape=(
            jax.ShapeDtypeStruct((blocks, 128, 2 * ROWS), jnp.float32),
            jax.ShapeDtypeStruct((2, blocks, 2 * ROWS), jnp.float32),
        ),
        in_specs=[pl.BlockSpec(memory_space=pltpu.SMEM)] + [vmem] * (2 + len(state)),
        out_specs=(vmem, vmem),
        scratch_shapes=[
            pltpu.VMEM((2 * N_CORE * ROWS, 128), jnp.bfloat16),
            pltpu.VMEM((128, N_CORE * ROWS), jnp.bfloat16),
            pltpu.VMEM((N_CORE * ROWS, 128), jnp.float32),
            pltpu.SMEM((2 + 2 * blocks,), jnp.float32),
        ],
        input_output_aliases={3: 0, 4: 1} if state else {},
        compiler_params=pltpu.CompilerParams(vmem_limit_bytes=VMEM_LIMIT),
        cost_estimate=pl.CostEstimate(
            flops=pairs * 512, transcendentals=pairs, bytes_accessed=blocks << 20
        ),
        name=f"attend_{step}",
    )(where, q_all, kv, *state)


def combine_kernel(factor, where_ref, lam_ref, acc_ref, ml_ref, *refs):
    others, outs = refs[: N_Y - 1], refs[N_Y - 1 :]
    blocks = acc_ref.shape[0]
    lam = jnp.where(where_ref[2] == 0, lam_ref[0], lam_ref[1])
    m_own = ml_ref[0]
    all_m, all_l = [m_own], [ml_ref[1]]
    for d, ref in enumerate(others, 1):
        shift = blocks - N_CORE * d
        all_m.append(pltpu.roll(ref[0], shift, 0))
        all_l.append(pltpu.roll(ref[1], shift, 0))
    top = functools.reduce(jnp.maximum, all_m)
    total = jnp.zeros_like(top)
    for m, l in zip(all_m, all_l):
        total = total + l * jnp.exp2((m - top) * factor)
    scale = jnp.exp2((m_own - top) * factor) / total
    lane = lax.broadcasted_iota(jnp.int32, scale.shape, 1)
    scale = jnp.where(lane < ROWS, scale, -lam * scale)
    for n in range(blocks):
        part = (
            acc_ref[n, :, 0:ROWS] * scale[n : n + 1, 0:ROWS]
            + acc_ref[n, :, ROWS : 2 * ROWS] * scale[n : n + 1, ROWS : 2 * ROWS]
        )
        outs[n // N_CORE][n % N_CORE] = part.astype(jnp.bfloat16)


def combine(factor, where, lam, acc, ml, others):
    smem, vmem = (pl.BlockSpec(memory_space=m) for m in (pltpu.SMEM, pltpu.VMEM))
    return pl.pallas_call(
        functools.partial(combine_kernel, factor),
        out_shape=[jax.ShapeDtypeStruct((N_CORE, 128, ROWS), jnp.bfloat16)] * N_Y,
        in_specs=[smem, smem, *([vmem] * (2 + len(others)))],
        out_specs=[vmem] * N_Y,
        compiler_params=pltpu.CompilerParams(vmem_limit_bytes=VMEM_LIMIT),
        cost_estimate=pl.CostEstimate(
            flops=8 * 128 * 4096, transcendentals=4096 * 5, bytes_accessed=3 << 20
        ),
        name="combine",
    )(where, lam, acc, ml, *others)


def merge_kernel(where_ref, gain_ref, *refs):
    out_ref = refs[-1]
    gains = jnp.where(where_ref[2] == 0, gain_ref[0:1], gain_ref[1:2])
    gain = jnp.transpose(jnp.broadcast_to(gains, (128, 128)))[:, 0:1]
    for half in range(N_CORE):
        heads = functools.reduce(jnp.add, [ref[half].astype(jnp.float32) for ref in refs[:-1]])
        mean = jnp.mean(heads * heads, axis=0, keepdims=True)
        normed = (heads * lax.rsqrt(mean + epsilon) * gain).astype(jnp.bfloat16)
        for t in range(TP):
            out_ref[t * N_CORE + half] = normed


def merge(where, gain, sources):
    smem, vmem = (pl.BlockSpec(memory_space=m) for m in (pltpu.SMEM, pltpu.VMEM))
    return pl.pallas_call(
        merge_kernel,
        out_shape=jax.ShapeDtypeStruct((TP * N_CORE, 128, ROWS), jnp.bfloat16),
        in_specs=[smem, vmem, *([vmem] * len(sources))],
        out_specs=vmem,
        compiler_params=pltpu.CompilerParams(vmem_limit_bytes=VMEM_LIMIT),
        cost_estimate=pl.CostEstimate(
            flops=8 * 128 * 1024, transcendentals=1024, bytes_accessed=1 << 20
        ),
        name="merge",
    )(where, gain, *sources)


def round_by(array, axis, by):
    length = lax.axis_size(axis)
    return lax.ppermute(array, axis, [(i, (i + by) % length) for i in range(length)])


def per_device(
    residual,
    queries,
    keys,
    values,
    documents,
    lambdas,
    head_gain,
    out_weight,
    mix_gain,
    pre_gain,
    gate_weight,
    value_weight,
    gate_taps,
    value_taps,
    down_weight,
    mlp_gain,
):
    tok_rows = residual.shape[0]
    score_scale = (queries.shape[2] // 2) ** (-0.5)
    factor = score_scale * math.log2(math.e)
    z_at, y_at, core = lax.axis_index("z"), lax.axis_index("y"), lax.axis_index("c")
    where = jnp.stack([z_at, y_at, core]).astype(jnp.int32)

    doc_rows = documents.reshape(2, 128).astype(jnp.bfloat16)
    tail = jnp.pad(
        jnp.concatenate([doc_rows, doc_rows], axis=1), ((0, EXTRA - 2), (0, 128))
    )
    values_across = jnp.transpose(
        values.reshape(2, 128, N_CORE, 128), (2, 0, 3, 1)
    ).reshape(N_CORE, tok_rows, 128)
    rows = [jnp.transpose(a, (1, 0, 2)) for a in (queries, keys)] + [values_across]
    both = jnp.concatenate(
        [jnp.concatenate(rows, axis=2), jnp.broadcast_to(tail, (N_CORE, EXTRA, 384))], axis=1
    )
    held = lax.all_to_all(both, "c", 0, 0, tiled=True)
    weights = lax.all_gather(
        jnp.concatenate([gate_weight, value_weight, down_weight], axis=1), SEQ, axis=0, tiled=True
    )
    q_own, kv = held[:, :, 0:128], held[:, :, 128:384]

    planes = SPAN // (tok_rows * N_Y * N_CORE)
    q_all = jnp.concatenate([q_own, *(round_by(q_own, "y", r) for r in range(1, N_Y))], axis=0)
    state = ()
    older = None
    for step in range(planes + 1):
        if step < planes:
            if step > 1:
                kv, _ = lax.optimization_barrier((kv, older))
            coming = round_by(kv, "z", 1)
        older = state
        state = attend(step, factor, where, q_all, kv, state)
        kv = coming
    acc, ml = state
    others = [round_by(ml, "y", -d) for d in range(1, N_Y)]
    parts = combine(factor, where, lambdas, acc, ml, others)
    sources = [parts[0], *(round_by(parts[r], "y", -r) for r in (2, 1, 3))]
    spread = merge(where, head_gain, sources)
    all_heads = lax.all_to_all(spread, ("tp", "c"), 0, 0, tiled=True).reshape(-1, tok_rows)
    mixed = lax.dot_general(
        all_heads, out_weight, (((0,), (0,)), ((), ())), preferred_element_type=jnp.float32
    )
    stream = residual.astype(jnp.float32) + rms_scale(mixed, mix_gain)
    normal_input = rms_scale(stream, pre_gain).astype(jnp.bfloat16)

    hidden_units = gate_weight.shape[1]
    reach = gate_taps.shape[0] - 1
    rim = jnp.concatenate(
        [
            normal_input[tok_rows - reach :],
            jnp.broadcast_to(doc_rows[1, 128 - reach :, None], (reach, 128)),
        ],
        axis=1,
    )
    length = lax.axis_size(SEQ)
    rim = lax.ppermute(rim, SEQ, [(i, i + 1) for i in range(length - 1)])
    features = normal_input.shape[1]
    earlier_docs = jnp.concatenate([rim[:, features].astype(jnp.int32), documents])
    extended_input, weights = lax.optimization_barrier(
        (jnp.concatenate([rim[:, 0:features], normal_input]), weights)
    )
    pre = jnp.dot(
        extended_input, weights[:, 0 : 2 * hidden_units], preferred_element_type=jnp.float32
    ).astype(jnp.bfloat16)

    taps = jnp.concatenate([gate_taps, value_taps], axis=1)
    extended = lax.optimization_barrier(pre).astype(jnp.float32)
    summed = jnp.zeros((tok_rows, 2 * hidden_units), jnp.float32)
    for shift_by in range(reach + 1):
        same_doc = (earlier_docs[shift_by : shift_by + tok_rows] == documents)[:, None]
        summed = summed + jnp.where(
            same_doc, taps[shift_by][None, :] * extended[shift_by : shift_by + tok_rows], 0.0
        )
    hidden = (
        jax.nn.gelu(summed[:, 0:hidden_units], approximate=True) * summed[:, hidden_units:]
    ).astype(jnp.bfloat16)
    down_terms = lax.dot_general(
        hidden,
        weights[:, 2 * hidden_units :],
        (((1,), (1,)), ((), ())),
        preferred_element_type=jnp.float32,
    ).astype(jnp.bfloat16)

    part = tok_rows // TP
    terms = lax.all_to_all(down_terms, "tp", 0, 0, tiled=True).reshape(TP, part, -1)
    lifted = jnp.sum(terms.astype(jnp.float32), axis=0)
    own_stream = lax.dynamic_slice_in_dim(stream, lax.axis_index("tp") * part, part, 0)
    out = (own_stream + rms_scale(lifted, mlp_gain)).astype(jnp.bfloat16)
    copies = jnp.broadcast_to(out[None], (TP, *out.shape)).reshape(tok_rows, -1)
    return lax.all_to_all(copies, "tp", 0, 0, tiled=True)


def solution(mesh):
    devices = mesh.devices
    split = Mesh(
        devices.reshape(devices.shape[0] // (N_Y * N_CORE), N_Y, N_CORE, devices.shape[1]),
        ("z", "y", "c", "tp"),
    )
    placed = (
        P(SEQ, None),
        P(SEQ, "tp", None),
        P(SEQ, "tp", None),
        P(SEQ, "tp", None),
        P(SEQ),
        P("tp"),
        P("tp", None),
        P(),
        P(),
        P(),
        P(SEQ, "tp"),
        P(SEQ, "tp"),
        P(None, "tp"),
        P(None, "tp"),
        P(SEQ, "tp"),
        P(),
    )
    return jax.shard_map(
        per_device, mesh=split, in_specs=placed, out_specs=P(SEQ, None), check_vma=False
    )
```

```python
import functools
import math

import jax
import jax.numpy as jnp
from jax import lax
from jax.experimental import pallas as pl
from jax.experimental.pallas import tpu as pltpu
from jax.sharding import Mesh
from jax.sharding import PartitionSpec as P


epsilon = 1e-06
masked_score = -1e30
N_Y = 4
N_CORE = 2
TP = 4
SPAN = 8192
ROWS = 256
EXTRA = 16
SEQ = ("z", "y", "c")
VMEM_LIMIT = 16 << 20


def rms_scale(values_in, gain):
    return (
        values_in
        * lax.rsqrt(jnp.mean(values_in * values_in, axis=-1, keepdims=True) + epsilon)
        * gain
    )


def attend_kernel(first, step, factor, where_ref, q_ref, kv_ref, *refs):
    if first:
        old_acc = old_ml = None
    else:
        old_acc, old_ml = refs[:2]
        refs = refs[2:]
    new_acc, new_ml, qx_ref, vt_ref, kcol_ref, ends = refs
    blocks = new_acc.shape[0]
    z, y = where_ref[0], where_ref[1]
    key_plane = z - step
    keys = N_CORE * ROWS

    for b in range(N_CORE):
        for half in range(2):
            at = b * ROWS + half * 128
            vt_ref[:, at : at + 128] = kv_ref[b, half * 128 : half * 128 + 128, 128:256]
    tails = [kv_ref[b, ROWS : ROWS + EXTRA, 0:128].astype(jnp.float32) for b in range(N_CORE)]
    ends[0] = jnp.min(tails[0][0:1])
    ends[1] = jnp.max(tails[N_CORE - 1][1:2])
    for n in range(blocks):
        q_tail = q_ref[n, ROWS : ROWS + EXTRA, :].astype(jnp.float32)
        ends[2 + 2 * n] = jnp.min(q_tail[0:1])
        ends[3 + 2 * n] = jnp.max(q_tail[1:2])

    @pl.loop(0, N_Y)
    def _(r):
        from_y = lax.rem(y - r + N_Y, N_Y)
        q_index = (z * N_Y + from_y) * N_CORE
        k_index = (key_plane * N_Y + y) * N_CORE
        n0 = r * N_CORE
        q_first, q_last = ends[2 + 2 * n0], ends[1 + 2 * (n0 + N_CORE)]
        live = (key_plane >= 0) & (k_index <= q_index) & (ends[1] >= q_first)
        clean = (k_index < q_index) & (ends[0] == q_last)

        def update(masked):
            lane = lax.broadcasted_iota(jnp.int32, (ROWS, 128), 1)
            for h in range(N_CORE):
                queries = q_ref[n0 + h, 0:ROWS, :].astype(jnp.float32)
                at = h * 2 * ROWS
                qx_ref[at : at + ROWS] = jnp.where(lane < 64, queries, 0.0).astype(jnp.bfloat16)
                qx_ref[at + ROWS : at + 2 * ROWS] = jnp.where(lane < 64, 0.0, queries).astype(
                    jnp.bfloat16
                )
            key_rows = kv_ref[:, 0:ROWS, 0:128].reshape(keys, 128)
            if masked:
                for b in range(N_CORE):
                    docs = kv_ref[b, ROWS : ROWS + EXTRA, 0:128].astype(jnp.float32)
                    for half in range(2):
                        at = b * ROWS + half * 128
                        kcol_ref[at : at + 128] = jnp.transpose(
                            jnp.broadcast_to(docs[half : half + 1], (128, 128))
                        )
                row = lax.broadcasted_iota(jnp.int32, (keys, ROWS), 0)
                col = lax.broadcasted_iota(jnp.int32, (keys, ROWS), 1)
                key_docs = jnp.broadcast_to(kcol_ref[:, 0:1], (keys, ROWS))
            scores_of = [None] * (2 * N_CORE)

            def start(c):
                scores_of[c] = lax.dot_general(
                    key_rows,
                    qx_ref[c * ROWS : (c + 1) * ROWS],
                    (((1,), (1,)), ((), ())),
                    preferred_element_type=jnp.float32,
                )

            start(0)
            for c in range(2 * N_CORE):
                n, m = n0 + c // 2, c % 2
                this = pl.ds(n, 1)
                span = slice(m * ROWS, (m + 1) * ROWS)
                if c + 1 < 2 * N_CORE:
                    start(c + 1)
                scores = scores_of[c]
                if masked:
                    if m == 0:
                        q_tail = q_ref[n, ROWS : ROWS + EXTRA, :].astype(jnp.float32)
                        q_docs = jnp.concatenate([q_tail[0:1], q_tail[1:2]], axis=1)
                        ahead = (k_index - q_index - c // 2) * ROWS
                        allowed = (key_docs == q_docs) & (row + ahead <= col)
                    scores = jnp.where(allowed, scores, masked_score)
                new_max = jnp.max(scores, axis=0, keepdims=True)
                if not first:
                    old_max = old_ml[0, this, span]
                    new_max = jnp.maximum(old_max, new_max)
                    rescale = jnp.exp2((old_max - new_max) * factor)
                probs = jnp.exp2((scores - new_max) * factor)
                if masked:
                    probs = jnp.where(allowed, probs, 0.0)
                total = jnp.sum(probs, axis=0, keepdims=True)
                weighted = jnp.dot(
                    vt_ref[...], probs.astype(jnp.bfloat16), preferred_element_type=jnp.float32
                )
                if not first:
                    total = total + old_ml[1, this, span] * rescale
                    weighted = weighted + old_acc[n, :, span] * rescale
                new_ml[0, this, span] = new_max
                new_ml[1, this, span] = total
                new_acc[n, :, span] = weighted

        pl.when(live & clean)(functools.partial(update, False))
        pl.when(live & jnp.logical_not(clean))(functools.partial(update, True))

        @pl.when(jnp.logical_not(live))
        def _():
            for h in range(N_CORE):
                n = n0 + h
                this = pl.ds(n, 1)
                if first:
                    new_acc[n] = jnp.zeros(new_acc.shape[1:], jnp.float32)
                    new_ml[0, this] = jnp.full((1, 2 * ROWS), masked_score, jnp.float32)
                    new_ml[1, this] = jnp.zeros((1, 2 * ROWS), jnp.float32)
                else:
                    new_acc[n] = old_acc[n]
                    new_ml[0, this] = old_ml[0, this]
                    new_ml[1, this] = old_ml[1, this]


def attend(step, factor, where, q_all, kv, state):
    blocks = q_all.shape[0]
    vmem = pl.BlockSpec(memory_space=pltpu.VMEM)
    pairs = blocks * N_CORE * ROWS * 2 * ROWS
    return pl.pallas_call(
        functools.partial(attend_kernel, not state, step, factor),
        out_shape=(
            jax.ShapeDtypeStruct((blocks, 128, 2 * ROWS), jnp.float32),
            jax.ShapeDtypeStruct((2, blocks, 2 * ROWS), jnp.float32),
        ),
        in_specs=[pl.BlockSpec(memory_space=pltpu.SMEM)] + [vmem] * (2 + len(state)),
        out_specs=(vmem, vmem),
        scratch_shapes=[
            pltpu.VMEM((2 * N_CORE * ROWS, 128), jnp.bfloat16),
            pltpu.VMEM((128, N_CORE * ROWS), jnp.bfloat16),
            pltpu.VMEM((N_CORE * ROWS, 128), jnp.float32),
            pltpu.SMEM((2 + 2 * blocks,), jnp.float32),
        ],
        input_output_aliases={3: 0, 4: 1} if state else {},
        compiler_params=pltpu.CompilerParams(vmem_limit_bytes=VMEM_LIMIT),
        cost_estimate=pl.CostEstimate(
            flops=pairs * 512, transcendentals=pairs, bytes_accessed=blocks << 20
        ),
        name=f"attend_{step}",
    )(where, q_all, kv, *state)


def combine_kernel(factor, where_ref, lam_ref, acc_ref, ml_ref, *refs):
    others, outs = refs[: N_Y - 1], refs[N_Y - 1 :]
    blocks = acc_ref.shape[0]
    lam = jnp.where(where_ref[2] == 0, lam_ref[0], lam_ref[1])
    m_own = ml_ref[0]
    all_m, all_l = [m_own], [ml_ref[1]]
    for d, ref in enumerate(others, 1):
        shift = blocks - N_CORE * d
        all_m.append(pltpu.roll(ref[0], shift, 0))
        all_l.append(pltpu.roll(ref[1], shift, 0))
    top = functools.reduce(jnp.maximum, all_m)
    total = jnp.zeros_like(top)
    for m, l in zip(all_m, all_l):
        total = total + l * jnp.exp2((m - top) * factor)
    scale = jnp.exp2((m_own - top) * factor) / total
    lane = lax.broadcasted_iota(jnp.int32, scale.shape, 1)
    scale = jnp.where(lane < ROWS, scale, -lam * scale)
    for n in range(blocks):
        part = (
            acc_ref[n, :, 0:ROWS] * scale[n : n + 1, 0:ROWS]
            + acc_ref[n, :, ROWS : 2 * ROWS] * scale[n : n + 1, ROWS : 2 * ROWS]
        )
        outs[n // N_CORE][n % N_CORE] = part.astype(jnp.bfloat16)


def combine(factor, where, lam, acc, ml, others):
    smem, vmem = (pl.BlockSpec(memory_space=m) for m in (pltpu.SMEM, pltpu.VMEM))
    return pl.pallas_call(
        functools.partial(combine_kernel, factor),
        out_shape=[jax.ShapeDtypeStruct((N_CORE, 128, ROWS), jnp.bfloat16)] * N_Y,
        in_specs=[smem, smem, *([vmem] * (2 + len(others)))],
        out_specs=[vmem] * N_Y,
        compiler_params=pltpu.CompilerParams(vmem_limit_bytes=VMEM_LIMIT),
        cost_estimate=pl.CostEstimate(
            flops=8 * 128 * 4096, transcendentals=4096 * 5, bytes_accessed=3 << 20
        ),
        name="combine",
    )(where, lam, acc, ml, *others)


def merge_kernel(where_ref, gain_ref, *refs):
    out_ref = refs[-1]
    gains = jnp.where(where_ref[2] == 0, gain_ref[0:1], gain_ref[1:2])
    gain = jnp.transpose(jnp.broadcast_to(gains, (128, 128)))[:, 0:1]
    for half in range(N_CORE):
        heads = functools.reduce(jnp.add, [ref[half].astype(jnp.float32) for ref in refs[:-1]])
        mean = jnp.mean(heads * heads, axis=0, keepdims=True)
        normed = (heads * lax.rsqrt(mean + epsilon) * gain).astype(jnp.bfloat16)
        for t in range(TP):
            out_ref[t * N_CORE + half] = normed


def merge(where, gain, sources):
    smem, vmem = (pl.BlockSpec(memory_space=m) for m in (pltpu.SMEM, pltpu.VMEM))
    return pl.pallas_call(
        merge_kernel,
        out_shape=jax.ShapeDtypeStruct((TP * N_CORE, 128, ROWS), jnp.bfloat16),
        in_specs=[smem, vmem, *([vmem] * len(sources))],
        out_specs=vmem,
        compiler_params=pltpu.CompilerParams(vmem_limit_bytes=VMEM_LIMIT),
        cost_estimate=pl.CostEstimate(
            flops=8 * 128 * 1024, transcendentals=1024, bytes_accessed=1 << 20
        ),
        name="merge",
    )(where, gain, *sources)


def round_by(array, axis, by):
    length = lax.axis_size(axis)
    return lax.ppermute(array, axis, [(i, (i + by) % length) for i in range(length)])


def per_device(
    residual,
    queries,
    keys,
    values,
    documents,
    lambdas,
    head_gain,
    out_weight,
    mix_gain,
    pre_gain,
    gate_weight,
    value_weight,
    gate_taps,
    value_taps,
    down_weight,
    mlp_gain,
):
    tok_rows = residual.shape[0]
    score_scale = (queries.shape[2] // 2) ** (-0.5)
    factor = score_scale * math.log2(math.e)
    z_at, y_at, core = lax.axis_index("z"), lax.axis_index("y"), lax.axis_index("c")
    where = jnp.stack([z_at, y_at, core]).astype(jnp.int32)

    doc_rows = documents.reshape(2, 128).astype(jnp.bfloat16)
    tail = jnp.pad(
        jnp.concatenate([doc_rows, doc_rows], axis=1), ((0, EXTRA - 2), (0, 128))
    )
    values_across = jnp.transpose(
        values.reshape(2, 128, N_CORE, 128), (2, 0, 3, 1)
    ).reshape(N_CORE, tok_rows, 128)
    rows = [jnp.transpose(a, (1, 0, 2)) for a in (queries, keys)] + [values_across]
    both = jnp.concatenate(
        [jnp.concatenate(rows, axis=2), jnp.broadcast_to(tail, (N_CORE, EXTRA, 384))], axis=1
    )
    held = lax.all_to_all(both, "c", 0, 0, tiled=True)
    shards, held = lax.optimization_barrier(((gate_weight, value_weight, down_weight), held))
    weights = lax.all_gather(jnp.concatenate(shards, axis=1), SEQ, axis=0, tiled=True)
    q_own, kv = held[:, :, 0:128], held[:, :, 128:384]

    planes = SPAN // (tok_rows * N_Y * N_CORE)
    q_all = jnp.concatenate([q_own, *(round_by(q_own, "y", r) for r in range(1, N_Y))], axis=0)
    state = ()
    older = None
    for step in range(planes + 1):
        if step < planes:
            if step > 1:
                kv, _ = lax.optimization_barrier((kv, older))
            coming = round_by(kv, "z", 1)
        older = state
        state = attend(step, factor, where, q_all, kv, state)
        kv = coming
    acc, ml = state
    others = [round_by(ml, "y", -d) for d in range(1, N_Y)]
    parts = combine(factor, where, lambdas, acc, ml, others)
    sources = [parts[0], *(round_by(parts[r], "y", -r) for r in (2, 1, 3))]
    spread = merge(where, head_gain, sources)
    all_heads = lax.all_to_all(spread, ("tp", "c"), 0, 0, tiled=True).reshape(-1, tok_rows)
    mixed = lax.dot_general(
        all_heads, out_weight, (((0,), (0,)), ((), ())), preferred_element_type=jnp.float32
    )
    stream = residual.astype(jnp.float32) + rms_scale(mixed, mix_gain)
    normal_input = rms_scale(stream, pre_gain).astype(jnp.bfloat16)

    hidden_units = gate_weight.shape[1]
    reach = gate_taps.shape[0] - 1
    rim = jnp.concatenate(
        [
            normal_input[tok_rows - reach :],
            jnp.broadcast_to(doc_rows[1, 128 - reach :, None], (reach, 128)),
        ],
        axis=1,
    )
    length = lax.axis_size(SEQ)
    rim = lax.ppermute(rim, SEQ, [(i, i + 1) for i in range(length - 1)])
    features = normal_input.shape[1]
    earlier_docs = jnp.concatenate([rim[:, features].astype(jnp.int32), documents])
    extended_input, weights = lax.optimization_barrier(
        (jnp.concatenate([rim[:, 0:features], normal_input]), weights)
    )
    pre = jnp.dot(
        extended_input, weights[:, 0 : 2 * hidden_units], preferred_element_type=jnp.float32
    ).astype(jnp.bfloat16)

    taps = jnp.concatenate([gate_taps, value_taps], axis=1)
    extended = lax.optimization_barrier(pre).astype(jnp.float32)
    summed = jnp.zeros((tok_rows, 2 * hidden_units), jnp.float32)
    for shift_by in range(reach + 1):
        same_doc = (earlier_docs[shift_by : shift_by + tok_rows] == documents)[:, None]
        summed = summed + jnp.where(
            same_doc, taps[shift_by][None, :] * extended[shift_by : shift_by + tok_rows], 0.0
        )
    hidden = (
        jax.nn.gelu(summed[:, 0:hidden_units], approximate=True) * summed[:, hidden_units:]
    ).astype(jnp.bfloat16)
    down_terms = lax.dot_general(
        hidden,
        weights[:, 2 * hidden_units :],
        (((1,), (1,)), ((), ())),
        preferred_element_type=jnp.float32,
    ).astype(jnp.bfloat16)

    part = tok_rows // TP
    terms = lax.all_to_all(down_terms, "tp", 0, 0, tiled=True).reshape(TP, part, -1)
    lifted = jnp.sum(terms.astype(jnp.float32), axis=0)
    own_stream = lax.dynamic_slice_in_dim(stream, lax.axis_index("tp") * part, part, 0)
    out = (own_stream + rms_scale(lifted, mlp_gain)).astype(jnp.bfloat16)
    copies = jnp.broadcast_to(out[None], (TP, *out.shape)).reshape(tok_rows, -1)
    return lax.all_to_all(copies, "tp", 0, 0, tiled=True)


def solution(mesh):
    devices = mesh.devices
    split = Mesh(
        devices.reshape(devices.shape[0] // (N_Y * N_CORE), N_Y, N_CORE, devices.shape[1]),
        ("z", "y", "c", "tp"),
    )
    placed = (
        P(SEQ, None),
        P(SEQ, "tp", None),
        P(SEQ, "tp", None),
        P(SEQ, "tp", None),
        P(SEQ),
        P("tp"),
        P("tp", None),
        P(),
        P(),
        P(),
        P(SEQ, "tp"),
        P(SEQ, "tp"),
        P(None, "tp"),
        P(None, "tp"),
        P(SEQ, "tp"),
        P(),
    )
    return jax.shard_map(
        per_device, mesh=split, in_specs=placed, out_specs=P(SEQ, None), check_vma=False
    )
```

```python
import functools
import math

import jax
import jax.numpy as jnp
from jax import lax
from jax.experimental import pallas as pl
from jax.experimental.pallas import tpu as pltpu
from jax.sharding import Mesh
from jax.sharding import PartitionSpec as P


epsilon = 1e-06
masked_score = -1e30
N_Y = 4
N_CORE = 2
TP = 4
SPAN = 8192
ROWS = 256
EXTRA = 8
SEQ = ("z", "y", "c")
VMEM_LIMIT = 16 << 20


def rms_scale(values_in, gain):
    return (
        values_in
        * lax.rsqrt(jnp.mean(values_in * values_in, axis=-1, keepdims=True) + epsilon)
        * gain
    )


def attend_kernel(first, step, factor, where_ref, q_ref, kv_ref, *refs):
    if first:
        old_acc = old_ml = None
    else:
        old_acc, old_ml = refs[:2]
        refs = refs[2:]
    new_acc, new_ml, qx_ref, vt_ref, kcol_ref, ends = refs
    blocks = new_acc.shape[0]
    z, y = where_ref[0], where_ref[1]
    key_plane = z - step
    keys = N_CORE * ROWS

    for b in range(N_CORE):
        for half in range(2):
            at = b * ROWS + half * 128
            vt_ref[:, at : at + 128] = kv_ref[b, half * 128 : half * 128 + 128, 128:256]
    tails = [kv_ref[b, ROWS : ROWS + EXTRA, 0:128].astype(jnp.float32) for b in range(N_CORE)]
    ends[0] = jnp.min(tails[0][0:1])
    ends[1] = jnp.max(tails[N_CORE - 1][1:2])
    for n in range(blocks):
        q_tail = q_ref[n, ROWS : ROWS + EXTRA, :].astype(jnp.float32)
        ends[2 + 2 * n] = jnp.min(q_tail[0:1])
        ends[3 + 2 * n] = jnp.max(q_tail[1:2])

    @pl.loop(0, N_Y)
    def _(r):
        from_y = lax.rem(y - r + N_Y, N_Y)
        q_index = (z * N_Y + from_y) * N_CORE
        k_index = (key_plane * N_Y + y) * N_CORE
        n0 = r * N_CORE
        q_first, q_last = ends[2 + 2 * n0], ends[1 + 2 * (n0 + N_CORE)]
        live = (key_plane >= 0) & (k_index <= q_index) & (ends[1] >= q_first)
        clean = (k_index < q_index) & (ends[0] == q_last)

        def update(masked):
            lane = lax.broadcasted_iota(jnp.int32, (ROWS, 128), 1)
            for h in range(N_CORE):
                queries = q_ref[n0 + h, 0:ROWS, :].astype(jnp.float32)
                at = h * 2 * ROWS
                qx_ref[at : at + ROWS] = jnp.where(lane < 64, queries, 0.0).astype(jnp.bfloat16)
                qx_ref[at + ROWS : at + 2 * ROWS] = jnp.where(lane < 64, 0.0, queries).astype(
                    jnp.bfloat16
                )
            key_rows = kv_ref[:, 0:ROWS, 0:128].reshape(keys, 128)
            if masked:
                for b in range(N_CORE):
                    docs = kv_ref[b, ROWS : ROWS + EXTRA, 0:128].astype(jnp.float32)
                    for half in range(2):
                        at = b * ROWS + half * 128
                        kcol_ref[at : at + 128] = jnp.transpose(
                            jnp.broadcast_to(docs[half : half + 1], (128, 128))
                        )
                row = lax.broadcasted_iota(jnp.int32, (keys, ROWS), 0)
                col = lax.broadcasted_iota(jnp.int32, (keys, ROWS), 1)
                key_docs = jnp.broadcast_to(kcol_ref[:, 0:1], (keys, ROWS))
            scores_of = [None] * (2 * N_CORE)

            def start(c):
                scores_of[c] = lax.dot_general(
                    key_rows,
                    qx_ref[c * ROWS : (c + 1) * ROWS],
                    (((1,), (1,)), ((), ())),
                    preferred_element_type=jnp.float32,
                )

            start(0)
            for c in range(2 * N_CORE):
                n, m = n0 + c // 2, c % 2
                this = pl.ds(n, 1)
                span = slice(m * ROWS, (m + 1) * ROWS)
                if c + 1 < 2 * N_CORE:
                    start(c + 1)
                scores = scores_of[c]
                if masked:
                    if m == 0:
                        q_tail = q_ref[n, ROWS : ROWS + EXTRA, :].astype(jnp.float32)
                        q_docs = jnp.concatenate([q_tail[0:1], q_tail[1:2]], axis=1)
                        ahead = (k_index - q_index - c // 2) * ROWS
                        allowed = (key_docs == q_docs) & (row + ahead <= col)
                    scores = jnp.where(allowed, scores, masked_score)
                new_max = jnp.max(scores, axis=0, keepdims=True)
                if not first:
                    old_max = old_ml[0, this, span]
                    new_max = jnp.maximum(old_max, new_max)
                    rescale = jnp.exp2((old_max - new_max) * factor)
                probs = jnp.exp2((scores - new_max) * factor)
                if masked:
                    probs = jnp.where(allowed, probs, 0.0)
                total = jnp.sum(probs, axis=0, keepdims=True)
                weighted = jnp.dot(
                    vt_ref[...], probs.astype(jnp.bfloat16), preferred_element_type=jnp.float32
                )
                if not first:
                    total = total + old_ml[1, this, span] * rescale
                    weighted = weighted + old_acc[n, :, span] * rescale
                new_ml[0, this, span] = new_max
                new_ml[1, this, span] = total
                new_acc[n, :, span] = weighted

        pl.when(live & clean)(functools.partial(update, False))
        pl.when(live & jnp.logical_not(clean))(functools.partial(update, True))

        @pl.when(jnp.logical_not(live))
        def _():
            for h in range(N_CORE):
                n = n0 + h
                this = pl.ds(n, 1)
                if first:
                    new_acc[n] = jnp.zeros(new_acc.shape[1:], jnp.float32)
                    new_ml[0, this] = jnp.full((1, 2 * ROWS), masked_score, jnp.float32)
                    new_ml[1, this] = jnp.zeros((1, 2 * ROWS), jnp.float32)
                else:
                    new_acc[n] = old_acc[n]
                    new_ml[0, this] = old_ml[0, this]
                    new_ml[1, this] = old_ml[1, this]


def attend(step, factor, where, q_all, kv, state):
    blocks = q_all.shape[0]
    vmem = pl.BlockSpec(memory_space=pltpu.VMEM)
    pairs = blocks * N_CORE * ROWS * 2 * ROWS
    return pl.pallas_call(
        functools.partial(attend_kernel, not state, step, factor),
        out_shape=(
            jax.ShapeDtypeStruct((blocks, 128, 2 * ROWS), jnp.float32),
            jax.ShapeDtypeStruct((2, blocks, 2 * ROWS), jnp.float32),
        ),
        in_specs=[pl.BlockSpec(memory_space=pltpu.SMEM)] + [vmem] * (2 + len(state)),
        out_specs=(vmem, vmem),
        scratch_shapes=[
            pltpu.VMEM((2 * N_CORE * ROWS, 128), jnp.bfloat16),
            pltpu.VMEM((128, N_CORE * ROWS), jnp.bfloat16),
            pltpu.VMEM((N_CORE * ROWS, 128), jnp.float32),
            pltpu.SMEM((2 + 2 * blocks,), jnp.float32),
        ],
        input_output_aliases={3: 0, 4: 1} if state else {},
        compiler_params=pltpu.CompilerParams(vmem_limit_bytes=VMEM_LIMIT),
        cost_estimate=pl.CostEstimate(
            flops=pairs * 512, transcendentals=pairs, bytes_accessed=blocks << 20
        ),
        name=f"attend_{step}",
    )(where, q_all, kv, *state)


def combine_kernel(factor, where_ref, lam_ref, acc_ref, ml_ref, *refs):
    others, outs = refs[: N_Y - 1], refs[N_Y - 1 :]
    blocks = acc_ref.shape[0]
    lam = jnp.where(where_ref[2] == 0, lam_ref[0], lam_ref[1])
    m_own = ml_ref[0]
    all_m, all_l = [m_own], [ml_ref[1]]
    for d, ref in enumerate(others, 1):
        shift = blocks - N_CORE * d
        all_m.append(pltpu.roll(ref[0], shift, 0))
        all_l.append(pltpu.roll(ref[1], shift, 0))
    top = functools.reduce(jnp.maximum, all_m)
    total = jnp.zeros_like(top)
    for m, l in zip(all_m, all_l):
        total = total + l * jnp.exp2((m - top) * factor)
    scale = jnp.exp2((m_own - top) * factor) / total
    lane = lax.broadcasted_iota(jnp.int32, scale.shape, 1)
    scale = jnp.where(lane < ROWS, scale, -lam * scale)
    for n in range(blocks):
        part = (
            acc_ref[n, :, 0:ROWS] * scale[n : n + 1, 0:ROWS]
            + acc_ref[n, :, ROWS : 2 * ROWS] * scale[n : n + 1, ROWS : 2 * ROWS]
        )
        outs[n // N_CORE][n % N_CORE] = part.astype(jnp.bfloat16)


def combine(factor, where, lam, acc, ml, others):
    smem, vmem = (pl.BlockSpec(memory_space=m) for m in (pltpu.SMEM, pltpu.VMEM))
    return pl.pallas_call(
        functools.partial(combine_kernel, factor),
        out_shape=[jax.ShapeDtypeStruct((N_CORE, 128, ROWS), jnp.bfloat16)] * N_Y,
        in_specs=[smem, smem, *([vmem] * (2 + len(others)))],
        out_specs=[vmem] * N_Y,
        compiler_params=pltpu.CompilerParams(vmem_limit_bytes=VMEM_LIMIT),
        cost_estimate=pl.CostEstimate(
            flops=8 * 128 * 4096, transcendentals=4096 * 5, bytes_accessed=3 << 20
        ),
        name="combine",
    )(where, lam, acc, ml, *others)


def merge_kernel(where_ref, gain_ref, *refs):
    out_ref = refs[-1]
    gains = jnp.where(where_ref[2] == 0, gain_ref[0:1], gain_ref[1:2])
    gain = jnp.transpose(jnp.broadcast_to(gains, (128, 128)))[:, 0:1]
    for half in range(N_CORE):
        heads = functools.reduce(jnp.add, [ref[half].astype(jnp.float32) for ref in refs[:-1]])
        mean = jnp.mean(heads * heads, axis=0, keepdims=True)
        normed = (heads * lax.rsqrt(mean + epsilon) * gain).astype(jnp.bfloat16)
        for t in range(TP):
            out_ref[t * N_CORE + half] = normed


def merge(where, gain, sources):
    smem, vmem = (pl.BlockSpec(memory_space=m) for m in (pltpu.SMEM, pltpu.VMEM))
    return pl.pallas_call(
        merge_kernel,
        out_shape=jax.ShapeDtypeStruct((TP * N_CORE, 128, ROWS), jnp.bfloat16),
        in_specs=[smem, vmem, *([vmem] * len(sources))],
        out_specs=vmem,
        compiler_params=pltpu.CompilerParams(vmem_limit_bytes=VMEM_LIMIT),
        cost_estimate=pl.CostEstimate(
            flops=8 * 128 * 1024, transcendentals=1024, bytes_accessed=1 << 20
        ),
        name="merge",
    )(where, gain, *sources)


def round_by(array, axis, by):
    length = lax.axis_size(axis)
    return lax.ppermute(array, axis, [(i, (i + by) % length) for i in range(length)])


def per_device(
    residual,
    queries,
    keys,
    values,
    documents,
    lambdas,
    head_gain,
    out_weight,
    mix_gain,
    pre_gain,
    gate_weight,
    value_weight,
    gate_taps,
    value_taps,
    down_weight,
    mlp_gain,
):
    tok_rows = residual.shape[0]
    score_scale = (queries.shape[2] // 2) ** (-0.5)
    factor = score_scale * math.log2(math.e)
    z_at, y_at, core = lax.axis_index("z"), lax.axis_index("y"), lax.axis_index("c")
    where = jnp.stack([z_at, y_at, core]).astype(jnp.int32)

    doc_rows = documents.reshape(2, 128).astype(jnp.bfloat16)
    tail = jnp.pad(
        jnp.concatenate([doc_rows, doc_rows], axis=1), ((0, EXTRA - 2), (0, 128))
    )
    values_across = jnp.transpose(
        values.reshape(2, 128, N_CORE, 128), (2, 0, 3, 1)
    ).reshape(N_CORE, tok_rows, 128)
    rows = [jnp.transpose(a, (1, 0, 2)) for a in (queries, keys)] + [values_across]
    both = jnp.concatenate(
        [jnp.concatenate(rows, axis=2), jnp.broadcast_to(tail, (N_CORE, EXTRA, 384))], axis=1
    )
    held = lax.all_to_all(both, "c", 0, 0, tiled=True)
    shards, held = lax.optimization_barrier(((gate_weight, value_weight, down_weight), held))
    weights = lax.all_gather(jnp.concatenate(shards, axis=1), SEQ, axis=0, tiled=True)
    q_own, kv = held[:, :, 0:128], held[:, :, 128:384]

    planes = SPAN // (tok_rows * N_Y * N_CORE)
    q_all = jnp.concatenate([q_own, *(round_by(q_own, "y", r) for r in range(1, N_Y))], axis=0)
    state = ()
    older = None
    for step in range(planes + 1):
        if step < planes:
            if step > 1:
                kv, _ = lax.optimization_barrier((kv, older))
            coming = round_by(kv, "z", 1)
        older = state
        state = attend(step, factor, where, q_all, kv, state)
        kv = coming
    acc, ml = state
    others = [round_by(ml, "y", -d) for d in range(1, N_Y)]
    parts = combine(factor, where, lambdas, acc, ml, others)
    sources = [parts[0], *(round_by(parts[r], "y", -r) for r in (2, 1, 3))]
    spread = merge(where, head_gain, sources)
    all_heads = lax.all_to_all(spread, ("tp", "c"), 0, 0, tiled=True).reshape(-1, tok_rows)
    mixed = lax.dot_general(
        all_heads, out_weight, (((0,), (0,)), ((), ())), preferred_element_type=jnp.float32
    )
    stream = residual.astype(jnp.float32) + rms_scale(mixed, mix_gain)
    normal_input = rms_scale(stream, pre_gain).astype(jnp.bfloat16)

    hidden_units = gate_weight.shape[1]
    reach = gate_taps.shape[0] - 1
    rim = jnp.concatenate(
        [
            normal_input[tok_rows - reach :],
            jnp.broadcast_to(doc_rows[1, 128 - reach :, None], (reach, 128)),
        ],
        axis=1,
    )
    length = lax.axis_size(SEQ)
    rim = lax.ppermute(rim, SEQ, [(i, i + 1) for i in range(length - 1)])
    features = normal_input.shape[1]
    earlier_docs = jnp.concatenate([rim[:, features].astype(jnp.int32), documents])
    extended_input, weights = lax.optimization_barrier(
        (jnp.concatenate([rim[:, 0:features], normal_input]), weights)
    )
    pre = jnp.dot(
        extended_input, weights[:, 0 : 2 * hidden_units], preferred_element_type=jnp.float32
    ).astype(jnp.bfloat16)

    taps = jnp.concatenate([gate_taps, value_taps], axis=1)
    extended = lax.optimization_barrier(pre).astype(jnp.float32)
    summed = jnp.zeros((tok_rows, 2 * hidden_units), jnp.float32)
    for shift_by in range(reach + 1):
        same_doc = (earlier_docs[shift_by : shift_by + tok_rows] == documents)[:, None]
        summed = summed + jnp.where(
            same_doc, taps[shift_by][None, :] * extended[shift_by : shift_by + tok_rows], 0.0
        )
    hidden = (
        jax.nn.gelu(summed[:, 0:hidden_units], approximate=True) * summed[:, hidden_units:]
    ).astype(jnp.bfloat16)
    down_terms = lax.dot_general(
        hidden,
        weights[:, 2 * hidden_units :],
        (((1,), (1,)), ((), ())),
        preferred_element_type=jnp.float32,
    ).astype(jnp.bfloat16)

    part = tok_rows // TP
    terms = lax.all_to_all(down_terms, "tp", 0, 0, tiled=True).reshape(TP, part, -1)
    lifted = jnp.sum(terms.astype(jnp.float32), axis=0)
    own_stream = lax.dynamic_slice_in_dim(stream, lax.axis_index("tp") * part, part, 0)
    out = (own_stream + rms_scale(lifted, mlp_gain)).astype(jnp.bfloat16)
    copies = jnp.broadcast_to(out[None], (TP, *out.shape)).reshape(tok_rows, -1)
    return lax.all_to_all(copies, "tp", 0, 0, tiled=True)


def solution(mesh):
    devices = mesh.devices
    split = Mesh(
        devices.reshape(devices.shape[0] // (N_Y * N_CORE), N_Y, N_CORE, devices.shape[1]),
        ("z", "y", "c", "tp"),
    )
    placed = (
        P(SEQ, None),
        P(SEQ, "tp", None),
        P(SEQ, "tp", None),
        P(SEQ, "tp", None),
        P(SEQ),
        P("tp"),
        P("tp", None),
        P(),
        P(),
        P(),
        P(SEQ, "tp"),
        P(SEQ, "tp"),
        P(None, "tp"),
        P(None, "tp"),
        P(SEQ, "tp"),
        P(),
    )
    return jax.shard_map(
        per_device, mesh=split, in_specs=placed, out_specs=P(SEQ, None), check_vma=False
    )
```
